256 devices in a mesh: sp: 16 (over y, x), tp: 16 (over z, core).
Axes of the slice: x: 4, y: 4, z: 8, core: 2. Of those that a mesh axis runs over, the one named last changes fastest.
Arguments:
- conv_in: bfloat16 [1024, 65536], P('tp', 'sp'), may hold values from -6 to 6
- in_gate: bfloat16 [1024, 65536], P('tp', 'sp'), may hold values from -6 to 6
- out_gate: bfloat16 [1024, 65536], P('tp', 'sp'), may hold values from -6 to 6
- doc_ids: int32 [65536], P('sp'), may hold values from 0 to 7, never falling along the last dimension, each value on 1 to 12288 neighbouring positions
- conv_taps: float32 [1024, 3], P('tp'), may hold values from -3.5 to 3.5
- head_gain: float32 [1024], P('tp'), may hold values from 0.1 to 1.9
- out_proj: bfloat16 [1024, 2048], P('tp'), may hold values from -0.1875 to 0.1875
- resid: bfloat16 [65536, 2048], P(('sp', 'tp')), may hold values from -6 to 6
- norm_gain: float32 [2048], replicated, may hold values from 0.1 to 1.9
- route_ids: int32 [65536, 2], P(('sp', 'tp')), may hold values from 0 to 15, all different within a row; in each aligned block of 128 rows (0 to 127, 128 to 255, ...) at most 32 rows name the same one
- route_weight: float32 [65536, 2], P(('sp', 'tp')), may hold values from 0.1 to 1
- w_gate: bfloat16 [16, 2048, 512], P('sp'), may hold values from -0.125 to 0.125
- w_up: bfloat16 [16, 2048, 512], P('sp'), may hold values from -0.125 to 0.125
- w_down: bfloat16 [16, 512, 2048], P('sp'), may hold values from -0.25 to 0.25
Outputs:
- layer_out: bfloat16 [65536, 2048], P(('sp', 'tp'))
The draws below stay inside these ranges and needn't reach their ends.
Inputs may be any that keep to these rules, and one draw needn't show every extreme that they name: `doc_ids`: document numbers never fall along the sequence; every number from 0 to 7 is used; no document is longer than 12288 positions and one is exactly that long. `route_ids`: each position names 2 different experts. In every aligned block of 128 positions no expert is named by more than 32 positions, a bound that some block reaches.
All inputs are finite; a program needn't handle non-finite values.
Results may differ from the reference program's by a relative error of at most 0.0051.
Values may be sent and summed in bfloat16 or wider, within the bound.
No kernel may reach another device: no remote copies, remote signals or barrier semaphores. Data moves between devices by JAX's collectives and lax.ppermute only.
A program may use at most 64 MiB of HBM per device.

```python
import math
import jax
import jax.numpy as jnp
import numpy as np
from jax import lax

D = 2048
HEAD = 64
CONV_CH = 1024
EXPERTS = 16
FF = 512
TOPK = 2
TOK_DEV = 4096
SEQ = 65536
HALF = 128
SLOT = 32
DOCS = 8


def level_of(own_key, dims, split, least, high):
    loudness, own = 1.0, jax.random.fold_in(own_key, 6)
    for axis_at, parts in split:
        draws = jnp.exp(jax.random.uniform(jax.random.fold_in(own, axis_at), (parts,), jnp.float32, least / len(split), high / len(split)))
        loudness = loudness * jnp.repeat(draws, dims[axis_at] // parts).reshape([-1 if axis == axis_at else 1 for axis in range(len(dims))])
    return loudness


def profile(number_of, total, most, skew):
    loads = [(1 << 20) // math.isqrt(grade ** skew) + 1 for grade in range(2, number_of + 1)]
    rest, given = total - most - (number_of - 1), [1] * (number_of - 1)
    while rest > 0:
        candidates = [i for i in range(number_of - 1) if given[i] < most]
        pool, left = sum([loads[i] for i in candidates]), rest
        for i in candidates:
            more = min(most - given[i], max(1, left * loads[i] // pool), rest)
            given[i] = given[i] + more
            rest = rest - more
    return np.array([most] + given)


def ragged_sizes(own_key, count, total, bound, lean):
    if count == 2:
        one = jax.random.randint(own_key, (), max(1, total - bound), min(bound, total - 1) + 1)
        return jnp.stack([one, total - one])
    sizes = jnp.asarray(profile(count, total, bound, lean), jnp.int32)
    twos = (count - 1) // 2
    source_of, receiver = sizes[1:1 + 2 * twos:2], sizes[2:2 + 2 * twos:2]
    room = jnp.minimum(source_of - 1, bound - receiver)
    passed = jax.random.randint(jax.random.fold_in(own_key, 1), (twos,), 0, 1 << 20) % (room + 1)
    sizes = sizes.at[1:1 + 2 * twos:2].set(source_of - passed).at[2:2 + 2 * twos:2].set(receiver + passed)
    return sizes[jax.random.permutation(jax.random.fold_in(own_key, 2), count)]


def assign_block(own_key, own, number, rows, number_of, top, limit, skew):
    ranking = jax.random.permutation(own_key, number_of)
    packed, common = load_shares(number_of, rows * top, limit, skew, True), load_shares(number_of, rows * top, limit, skew, False)
    places = jnp.arange(number_of)

    def named(lengths, offset_by):
        used = int((lengths > 0).sum())
        fixed = max(1, used // 4)
        shifted = fixed + (places - fixed + offset_by * (used - fixed)) % max(1, number_of - fixed)
        return jnp.zeros((number_of,), jnp.int32).at[ranking[jnp.where(places < fixed, places, shifted)]].set(jnp.asarray(lengths, jnp.int32))

    lengths = jnp.where(number % 4 == 0, named(packed, number // 4), named(common, number - number // 4 - 1))
    mixed = jax.random.permutation(jax.random.fold_in(own, 3), number_of)
    source_of, receiver = mixed[0:number_of // 2 * 2:2], mixed[1:number_of // 2 * 2:2]
    slack = jnp.minimum(lengths[source_of] - 1, limit - lengths[receiver]) // 2
    slack = jnp.where((source_of == ranking[0]) | (receiver == ranking[0]) | (lengths[receiver] == 0), 0, jnp.maximum(slack, 0))
    shifted = jax.random.randint(jax.random.fold_in(own, 4), (number_of // 2,), 0, 1 << 20) % (slack + 1)
    lengths = lengths.at[source_of].add(-shifted).at[receiver].add(shifted)
    members = jnp.searchsorted(jnp.cumsum(lengths), jnp.arange(rows * top), side="right").astype(jnp.int32)
    listing = members.reshape(top, rows).T
    listing = listing[jax.random.permutation(jax.random.fold_in(own, 1), rows)]
    offset_by = jax.random.randint(jax.random.fold_in(own, 2), (rows, 1), 0, top)
    return jnp.take_along_axis(listing, (jnp.arange(top)[None, :] + offset_by) % top, axis=1)


def load_shares(number_of, total, reach, skew, full):
    weights = [(1 << 20) // math.isqrt(rank ** skew) + 1 for rank in range(1, number_of + 1)]
    largest = reach if full else min(reach, max(-(-total // number_of), total * weights[0] // sum(weights)))
    least = 1 if total - largest >= number_of - 1 else 0
    counts, rest = [largest] + [least] * (number_of - 1), total - largest - least * (number_of - 1)
    while rest > 0:
        movable = [i for i in range(1, number_of) if counts[i] < largest] or [i for i in range(1, number_of) if counts[i] < reach]
        mass, budget = sum([weights[i] for i in movable]), rest
        for i in movable:
            extra = min(reach - counts[i], max(1, budget * weights[i] // mass), rest)
            counts[i] = counts[i] + extra
            rest = rest - extra
    return np.array(counts)


def centred(stream_key, extent, scale, limit, shards=(), held_as=jnp.bfloat16):
    factor_of = level_of(stream_key, extent, shards, -0.22, 0.18) if shards else 1.0
    values = jax.random.normal(stream_key, extent, jnp.float32) * scale * factor_of
    return jnp.minimum(jnp.maximum(values, -limit), limit).astype(held_as)


def setup_inputs(seed: int = 0) -> dict:
    key_of = jax.random.split(jax.random.key(seed), 15)
    conv_in = centred(key_of[0], (CONV_CH, SEQ), 1.0, 6.0, ((0, 16), (1, 16)))
    in_gate = centred(key_of[1], (CONV_CH, SEQ), 1.0, 6.0, ((0, 16), (1, 16)))
    out_gate = centred(key_of[2], (CONV_CH, SEQ), 1.0, 6.0, ((0, 16), (1, 16)))
    doc_ids = jnp.searchsorted(jnp.cumsum(ragged_sizes(key_of[3], DOCS, SEQ, 3 * TOK_DEV, 0)), jnp.arange(SEQ), side="right").astype(jnp.int32)
    conv_taps = centred(key_of[4], (CONV_CH, 3), 3 ** -0.5, 3.5, ((0, 16),), jnp.float32)
    head_gain = jnp.clip(1.0 + 0.18 * jax.random.normal(key_of[5], (CONV_CH,), jnp.float32), 0.1, 1.9)
    out_proj = centred(key_of[6], (CONV_CH, D), CONV_CH ** -0.5, 0.1875, ((0, 16),))
    resid = centred(key_of[7], (SEQ, D), 1.0, 6.0, ((0, 256),))
    norm_gain = jnp.clip(1.0 + 0.18 * jax.random.normal(key_of[8], (D,), jnp.float32), 0.1, 1.9)
    route_ids_keys = jax.random.split(jax.random.fold_in(key_of[9], 1), SEQ // HALF)
    route_ids_turns = jax.random.permutation(jax.random.fold_in(key_of[9], 3), SEQ // HALF)
    route_ids = jax.vmap(lambda own, number: assign_block(jax.random.fold_in(key_of[9], 2), own, number, HALF, EXPERTS, TOPK, SLOT, 1))(route_ids_keys, route_ids_turns).reshape((SEQ, TOPK))
    route_weight = jnp.clip(0.1 + 0.9 * jax.random.uniform(key_of[10], (SEQ, TOPK), jnp.float32) ** level_of(key_of[10], (SEQ, TOPK), ((0, 256),), -0.2, 0.2), 0.1, 1.0)
    w_gate = centred(key_of[11], (EXPERTS, D, FF), D ** -0.5, 0.125, ((0, 16),))
    w_up = centred(key_of[12], (EXPERTS, D, FF), D ** -0.5, 0.125, ((0, 16),))
    w_down = centred(key_of[13], (EXPERTS, FF, D), FF ** -0.5, 0.25, ((0, 16),))
    return {"conv_in": conv_in, "in_gate": in_gate, "out_gate": out_gate, "doc_ids": doc_ids, "conv_taps": conv_taps, "head_gain": head_gain, "out_proj": out_proj, "resid": resid, "norm_gain": norm_gain, "route_ids": route_ids, "route_weight": route_weight, "w_gate": w_gate, "w_up": w_up, "w_down": w_down}


norm_eps = 1e-06

def reference(conv_in, in_gate, out_gate, doc_ids, conv_taps, head_gain, out_proj, resid, norm_gain, route_ids, route_weight, w_gate, w_up, w_down):
    gated_in = in_gate.astype(jnp.float32) * conv_in.astype(jnp.float32)
    channels = gated_in.shape[0]
    earlier = jnp.concatenate([jnp.full((2,), -1, jnp.int32), doc_ids.astype(jnp.int32)])
    same_one = (earlier[1:-1] == doc_ids).astype(jnp.float32)
    same_two = (earlier[:-2] == doc_ids).astype(jnp.float32)
    padded = jnp.concatenate([jnp.zeros((channels, 2), jnp.float32), gated_in], axis=1)
    conv_out = conv_taps[:, 2:3] * gated_in + conv_taps[:, 1:2] * (padded[:, 1:-1] * same_one) + conv_taps[:, 0:1] * (padded[:, :-2] * same_two)
    gated_out = out_gate.astype(jnp.float32) * conv_out
    by_head = gated_out.reshape(channels // HEAD, HEAD, -1)
    by_head = by_head * lax.rsqrt(lax.optimization_barrier(jnp.mean(by_head * by_head, axis=1, keepdims=True)) + norm_eps)
    head_normed = (by_head.reshape(channels, -1) * head_gain[:, None]).astype(jnp.bfloat16)
    mixed = jnp.dot(head_normed.astype(jnp.float32).T, out_proj.astype(jnp.float32))
    stream = resid.astype(jnp.float32) + mixed
    expert_in = (stream * lax.rsqrt(lax.optimization_barrier(jnp.mean(stream * stream, axis=1, keepdims=True)) + norm_eps) * norm_gain).astype(jnp.bfloat16)
    flat_ids = route_ids.reshape(-1).astype(jnp.int32)
    flat_tok = (jnp.arange(flat_ids.shape[0], dtype=jnp.int32) // TOPK).astype(jnp.int32)
    flat_weight = route_weight.reshape(-1)
    most_rows = min(SEQ, SLOT * (SEQ // HALF))

    def one_expert(totals, inputs):
        gate_mat, up_mat, down_mat, number = inputs
        ranked = jnp.argsort((flat_ids != number).astype(jnp.int32), stable=True)[:most_rows]
        picked = flat_tok[ranked]
        weight = jnp.where(flat_ids[ranked] == number, flat_weight[ranked], jnp.zeros_like(flat_weight[ranked]))
        sel_rows = expert_in[picked].astype(jnp.float32)
        gate_part = jnp.dot(sel_rows, gate_mat.astype(jnp.float32))
        up_part = jnp.dot(sel_rows, up_mat.astype(jnp.float32))
        hidden = (jax.nn.silu(gate_part) * up_part).astype(jnp.bfloat16)
        expert_out = jnp.dot(hidden.astype(jnp.float32), down_mat.astype(jnp.float32)).astype(jnp.bfloat16)
        return (totals.at[picked].add(expert_out.astype(jnp.float32) * weight[:, None]), None)
    totals, _ = lax.scan(one_expert, jnp.zeros(stream.shape, jnp.float32), (w_gate, w_up, w_down, jnp.arange(EXPERTS, dtype=jnp.int32)))
    return (stream + totals).astype(jnp.bfloat16)
```

```python
import functools

import jax
import jax.numpy as jnp
import numpy as np
from jax import lax
from jax.experimental import pallas as pl
from jax.experimental.pallas import tpu as pltpu
from jax.sharding import Mesh
from jax.sharding import PartitionSpec as P


HEAD = 64
EPS = 1e-06
ROWS = 256
HALF = 128
SLOT = 32
CHUNK = 64
WIDTH = 2048
FF = 512
SP = ("y", "x")
TP = ("z", "c")

GROUPS = (
    (((0, 0), "AB"), ((1, 0), "AB"), ((0, 1), "AB"), ((3, 0), "A"), ((0, 3), "A")),
    (((1, 1), "B"), ((3, 3), "A"), ((3, 1), "AB"), ((1, 3), "AB"), ((3, 2), "A"), ((2, 3), "A")),
)
FLAT = GROUPS[0] + GROUPS[1]
CHUNKS = [
    ((h[0] + (k == "B")) % 4, (h[1] + (k == "B")) % 4) for h, kinds in FLAT for k in kinds
]
assert len(set(CHUNKS)) == 16

VMEM = pl.BlockSpec(memory_space=pltpu.VMEM)
SMEM = pl.BlockSpec(memory_space=pltpu.SMEM)


def permute(value, axes, sizes, move):
    pairs = []
    for i in np.ndindex(*sizes):
        j = tuple(int(v) for v in np.mod(move(*i), sizes))
        pairs.append((int(np.ravel_multi_index(i, sizes)), int(np.ravel_multi_index(j, sizes))))
    return lax.ppermute(value, axes, pairs)


def by_chip(value, dy, dx):
    return permute(value, SP, (4, 4), lambda y, x: (y + dy, x + dx))


def along_z(value, step):
    return permute(value, "z", (8,), lambda z: (z + step,))


def swap_cores(value):
    return permute(value, "c", (2,), lambda c: (c + 1,))


def cost(flops, nbytes):
    return pl.CostEstimate(flops=int(flops), bytes_accessed=int(nbytes), transcendentals=0)


def conv_kernel(a_ref, b_ref, o_ref, m1_ref, m2_ref, halo_ref, taps_ref, gain_ref, out_ref):
    lane = lax.broadcasted_iota(jnp.int32, (HEAD, ROWS), 1)
    t0, t1, t2 = taps_ref[:, 0:1], taps_ref[:, 1:2], taps_ref[:, 2:3]
    gain = gain_ref[...]
    prev = halo_ref[...]
    p1, p2 = pltpu.roll(prev, 1, 1), pltpu.roll(prev, 2, 1)
    for t in range(16):
        at = slice(t * ROWS, (t + 1) * ROWS)
        g = a_ref[:, at].astype(jnp.float32) * b_ref[:, at].astype(jnp.float32)
        r1, r2 = pltpu.roll(g, 1, 1), pltpu.roll(g, 2, 1)
        g1 = jnp.where(lane < 1, p1, r1)
        g2 = jnp.where(lane < 2, p2, r2)
        conv = t2 * g + t1 * (g1 * m1_ref[:, at]) + t0 * (g2 * m2_ref[:, at])
        v = o_ref[:, at].astype(jnp.float32) * conv
        ms = jnp.sum(v * v, axis=0, keepdims=True) * (1.0 / HEAD)
        out_ref[t] = (v * lax.rsqrt(ms + EPS) * gain).astype(jnp.bfloat16)
        p1, p2 = r1, r2


def conv(conv_in, in_gate, out_gate, m1, m2, halo, taps, gain):
    return pl.pallas_call(
        conv_kernel,
        out_shape=jax.ShapeDtypeStruct((16, HEAD, ROWS), jnp.bfloat16),
        in_specs=[VMEM] * 8,
        out_specs=VMEM,
        compiler_params=pltpu.CompilerParams(vmem_limit_bytes=8 << 20),
        cost_estimate=cost(8e9, 2 << 20),
        name="conv",
    )(conv_in, in_gate, out_gate, m1, m2, halo, taps, gain)


OFFSETS = (0, -1, 1, -2, 2, -3, 3, -4)


def mix_kernel(where_ref, by_row_ref, *refs):
    n_own = len(OFFSETS)
    own = refs[:n_own]
    swapped = refs[n_own : n_own + 2]
    resid_ref, gain_ref, tgt_ref = refs[n_own + 2 : n_own + 5]
    stream_ref = refs[n_own + 5]
    outs = refs[n_own + 6 : n_own + 6 + len(FLAT)]
    lhs, rhs, table = refs[n_own + 6 + len(FLAT) :]
    z, c = where_ref[0], where_ref[1]
    for q, off in enumerate(OFFSETS):
        zz = lax.rem(z + (off + 8), 8)
        lhs[pl.ds(q * 64, 64), :] = by_row_ref[zz * 2 + c]
        lhs[pl.ds(512 + q * 64, 64), :] = by_row_ref[zz * 2 + 1 - c]
        rhs[pl.ds(q * 64, 64), :] = own[q][...]
    first = swapped[0].shape[0]
    rhs[pl.ds(512, first), :] = swapped[0][...]
    rhs[pl.ds(512 + first, 512 - first), :] = swapped[1][...]
    slot = lax.broadcasted_iota(jnp.int32, (CHUNK, ROWS), 0)
    for j in range(16):
        hit = slot == tgt_ref[j : j + 1, :]
        table[pl.ds(j * CHUNK, CHUNK), :] = jnp.where(hit, 1.0, 0.0).astype(jnp.bfloat16)
    tile = 512
    left = lhs[...]
    total = jnp.zeros((ROWS, 1), jnp.float32)
    for n in range(WIDTH // tile):
        at = slice(n * tile, (n + 1) * tile)
        mixed = lax.dot_general(
            left, rhs[:, at], (((0,), (0,)), ((), ())), preferred_element_type=jnp.float32
        )
        stream = resid_ref[:, at].astype(jnp.float32) + mixed
        stream_ref[:, at] = stream
        total = total + jnp.sum(stream * stream, axis=1, keepdims=True)
    scale = lax.rsqrt(total * (1.0 / WIDTH) + EPS)
    for n in range(WIDTH // tile):
        at = slice(n * tile, (n + 1) * tile)
        normed = (stream_ref[:, at] * scale * gain_ref[:, at]).astype(jnp.bfloat16)
        packed = jnp.dot(table[...], normed, preferred_element_type=jnp.float32)
        packed = packed.astype(jnp.bfloat16)
        row = 0
        for ref in outs:
            ref[:, at] = packed[row : row + ref.shape[0]]
            row += ref.shape[0]


def mix(where, by_row, own, swapped, resid, gain, tgt):
    shapes = [jax.ShapeDtypeStruct((ROWS, WIDTH), jnp.float32)] + [
        jax.ShapeDtypeStruct((CHUNK * len(kinds), WIDTH), jnp.bfloat16) for _, kinds in FLAT
    ]
    return pl.pallas_call(
        mix_kernel,
        out_shape=shapes,
        in_specs=[SMEM] + [VMEM] * (1 + len(own) + len(swapped) + 3),
        out_specs=[VMEM] * len(shapes),
        scratch_shapes=[
            pltpu.VMEM((1024, ROWS), jnp.bfloat16),
            pltpu.VMEM((1024, WIDTH), jnp.bfloat16),
            pltpu.VMEM((1024, ROWS), jnp.bfloat16),
        ],
        compiler_params=pltpu.CompilerParams(vmem_limit_bytes=36 << 20),
        cost_estimate=cost(2.2e9, 12 << 20),
        name="mix",
    )(where, by_row, *own, *swapped, resid, gain, tgt)


def expert_kernel(group, *refs):
    n = len(group)
    bufs = refs[:n]
    wg, wu, wd, pk0, pk1 = refs[n : n + 5]
    outs = refs[n + 5 : 2 * n + 5]
    xa, xb, acc = refs[2 * n + 5 :]
    step = pl.program_id(0)

    def places(kind):
        row, found = 0, []
        for i, (_, kinds) in enumerate(group):
            if kind in kinds:
                found.append((row, i, kinds.index(kind) * CHUNK))
                row += CHUNK
        return row, found

    rows_a, in_a = places("A")
    rows_b, in_b = places("B")

    def gated(x, gate, up):
        g = jnp.dot(x, gate, preferred_element_type=jnp.float32)
        u = jnp.dot(x, up, preferred_element_type=jnp.float32)
        return (g / (1.0 + jnp.exp(-g)) * u).astype(jnp.bfloat16)

    def down_own(h, part):
        return jnp.dot(h, part, preferred_element_type=jnp.float32)

    @pl.when(step == 0)
    def _():
        for ref, found in ((xa, in_a), (xb, in_b)):
            for row, i, at in found:
                ref[pl.ds(row, CHUNK), :] = bufs[i][pl.ds(at, CHUNK), :]
        h = gated(xa[...], wg[...], wu[...])
        acc[...] = jnp.dot(h, wd[...], preferred_element_type=jnp.float32)

    @pl.when(step == 1)
    def _():
        h = gated(xa[...], wg[...], wu[...])
        for n0 in range(0, WIDTH, 512):
            at = slice(n0, n0 + 512)
            y = acc[:, at] + jnp.dot(h, wd[:, at], preferred_element_type=jnp.float32)
            y = y.astype(jnp.bfloat16)
            for row, i, off in in_a:
                outs[i][pl.ds(off, CHUNK), at] = y[row : row + CHUNK]

    def partner(pk, last):
        h = gated(xb[...], pk[0:2048, :], pk[2048:4096, :])
        for j in range(8):
            at = slice(j * 256, (j + 1) * 256)
            y = jnp.dot(
                h, pk[4096 + j * 256 : 4352 + j * 256, :], preferred_element_type=jnp.float32
            )
            if not last:
                acc[:rows_b, at] = y
            else:
                y = (acc[:rows_b, at] + y).astype(jnp.bfloat16)
                for row, i, off in in_b:
                    outs[i][pl.ds(off, CHUNK), at] = y[row : row + CHUNK]

    @pl.when(step == 2)
    def _():
        partner(pk0, False)

    @pl.when(step == 3)
    def _():
        partner(pk1, True)


def experts(group, bufs, wg, wu, wd, pk0, pk1):
    whole = [pl.BlockSpec(b.shape, lambda i: (0, 0)) for b in bufs]
    kinds = "".join(k for _, k in group)
    rows_a, rows_b = kinds.count("A") * CHUNK, kinds.count("B") * CHUNK
    tile = FF // 2
    return pl.pallas_call(
        functools.partial(expert_kernel, group),
        grid=(4,),
        out_shape=[jax.ShapeDtypeStruct(b.shape, jnp.bfloat16) for b in bufs],
        in_specs=whole
        + [
            pl.BlockSpec((WIDTH, tile), lambda i: (0, jnp.minimum(i, 1))),
            pl.BlockSpec((WIDTH, tile), lambda i: (0, jnp.minimum(i, 1))),
            pl.BlockSpec((tile, WIDTH), lambda i: (jnp.minimum(i, 1), 0)),
            VMEM,
            VMEM,
        ],
        out_specs=whole,
        scratch_shapes=[
            pltpu.VMEM((rows_a, WIDTH), jnp.bfloat16),
            pltpu.VMEM((rows_b, WIDTH), jnp.bfloat16),
            pltpu.VMEM((rows_a, WIDTH), jnp.float32),
        ],
        compiler_params=pltpu.CompilerParams(
            vmem_limit_bytes=40 << 20, dimension_semantics=("arbitrary",)
        ),
        cost_estimate=cost(6.0 * 512 * WIDTH * FF, 18 << 20),
        name="experts",
    )(*bufs, wg, wu, wd, pk0, pk1)


def combine_kernel(first, n, acc_ref, place_ref, weight_ref, *refs):
    bufs = refs[:n]
    out_ref, rows = refs[n], refs[n + 1]
    row = 0
    for ref in bufs:
        rows[pl.ds(row, ref.shape[0]), :] = ref[...]
        row += ref.shape[0]
    slot = lax.broadcasted_iota(jnp.int32, (ROWS, row), 1) + first
    table = jnp.where(place_ref[:, 0:1] == slot, weight_ref[:, 0:1], 0.0) + jnp.where(
        place_ref[:, 1:2] == slot, weight_ref[:, 1:2], 0.0
    )
    high = table.astype(jnp.bfloat16)
    low = (table - high.astype(jnp.float32)).astype(jnp.bfloat16)
    total = jnp.dot(high, rows[...], preferred_element_type=jnp.float32) + jnp.dot(
        low, rows[...], preferred_element_type=jnp.float32
    )
    out_ref[...] = (acc_ref[...] + total).astype(out_ref.dtype)


def combine(first, acc, place, weight, bufs, dtype):
    tile = 512
    rows = sum(b.shape[0] for b in bufs)
    return pl.pallas_call(
        functools.partial(combine_kernel, first, len(bufs)),
        grid=(WIDTH // tile,),
        out_shape=jax.ShapeDtypeStruct((ROWS, WIDTH), dtype),
        in_specs=[
            pl.BlockSpec((ROWS, tile), lambda i: (0, i)),
            pl.BlockSpec((ROWS, 2), lambda i: (0, 0)),
            pl.BlockSpec((ROWS, 2), lambda i: (0, 0)),
        ]
        + [pl.BlockSpec((b.shape[0], tile), lambda i: (0, i)) for b in bufs],
        out_specs=pl.BlockSpec((ROWS, tile), lambda i: (0, i)),
        scratch_shapes=[pltpu.VMEM((rows, tile), jnp.bfloat16)],
        compiler_params=pltpu.CompilerParams(
            vmem_limit_bytes=16 << 20, dimension_semantics=("arbitrary",)
        ),
        cost_estimate=cost(4.0 * ROWS * rows * WIDTH, 6 << 20),
        name="combine",
    )(acc, place, weight, *bufs)


def body(
    conv_in,
    in_gate,
    out_gate,
    doc_ids,
    conv_taps,
    head_gain,
    out_proj,
    resid,
    norm_gain,
    route_ids,
    route_weight,
    w_gate,
    w_up,
    w_down,
):
    y, x, z, c = (lax.axis_index(a) for a in ("y", "x", "z", "c"))

    last = in_gate[:, -2:].astype(jnp.float32) * conv_in[:, -2:].astype(jnp.float32)
    doc_value = doc_ids.astype(jnp.float32)
    tail = jnp.concatenate([last, doc_value[None, -2:]], axis=0)
    halo = lax.ppermute(tail, SP, [(i, i + 1) for i in range(15)])

    plus, minus = [out_proj], [out_proj]
    for _ in range(4):
        plus.append(along_z(plus[-1], 1))
    for _ in range(3):
        minus.append(along_z(minus[-1], -1))
    own = [out_proj, plus[1], minus[1], plus[2], minus[2], plus[3], minus[3], plus[4]]
    swapped = [
        swap_cores(jnp.concatenate(own[:5], axis=0)),
        swap_cores(jnp.concatenate(own[5:], axis=0)),
    ]

    wg, wu, wd = w_gate[0], w_up[0], w_down[0]
    half = FF // 2
    wd_half = lax.dynamic_slice_in_dim(wd, c * half, half, axis=0)
    pack = jnp.concatenate(
        [
            lax.dynamic_slice_in_dim(wg, c * half, half, axis=1),
            lax.dynamic_slice_in_dim(wu, c * half, half, axis=1),
        ]
        + [wd_half[:, j * half : (j + 1) * half] for j in range(WIDTH // half)],
        axis=0,
    )
    partner0 = by_chip(pack, -1, -1)
    partner1 = swap_cores(partner0)

    doc_before = jnp.concatenate([halo[HEAD], doc_value])
    same_one = (doc_before[1:-1] == doc_value).astype(jnp.float32)[None]
    same_two = (doc_before[:-2] == doc_value).astype(jnp.float32)[None]
    before = jnp.pad(halo[:HEAD], ((0, 0), (ROWS - 2, 0)))
    head_normed = conv(
        conv_in, in_gate, out_gate, same_one, same_two, before, conv_taps, head_gain[:, None]
    )
    by_row = lax.all_to_all(head_normed, TP, split_axis=0, concat_axis=0, tiled=True)

    displaced = np.array(CHUNKS, np.int32)
    expert_of = ((y + displaced[:, 0]) % 4) * 4 + (x + displaced[:, 1]) % 4
    ids = route_ids.T
    at0 = ids[0:1] == expert_of[:, None]
    at1 = ids[1:2] == expert_of[:, None]
    named = at0 | at1
    position = np.arange(ROWS)
    earlier = (position[:, None] < position[None, :]) & (
        position[:, None] // HALF == position[None, :] // HALF
    )
    rank = jnp.dot(
        named.astype(jnp.bfloat16),
        jnp.asarray(earlier, jnp.bfloat16),
        preferred_element_type=jnp.float32,
    ).astype(jnp.int32)
    in_chunk = rank + jnp.asarray(position // HALF * SLOT, jnp.int32)[None]
    tgt = jnp.where(named, in_chunk, -1)
    in_all = in_chunk + jnp.arange(16, dtype=jnp.int32)[:, None] * CHUNK
    place = jnp.stack(
        [jnp.sum(jnp.where(at, in_all, 0), axis=0) for at in (at0, at1)], axis=1
    )

    where = jnp.stack([z, c]).astype(jnp.int32)
    stream, *sends = mix(where, by_row, own, swapped, resid, norm_gain[None], tgt)

    arrived, k = [], 0
    for group in GROUPS:
        bufs = []
        for (dy, dx), _ in group:
            bufs.append(sends[k] if (dy, dx) == (0, 0) else by_chip(sends[k], dy, dx))
            k += 1
        arrived.append(bufs)
    total, first = stream, 0
    back = []
    for group, bufs in zip(GROUPS, arrived):
        results = experts(group, bufs, wg, wu, wd, partner0, partner1)
        back.append(
            [
                r if (dy, dx) == (0, 0) else by_chip(r, -dy, -dx)
                for r, ((dy, dx), _) in zip(results, group)
            ]
        )
    for n, bufs in enumerate(back):
        final = n == len(back) - 1
        total = combine(
            first, total, place, route_weight, bufs, jnp.bfloat16 if final else jnp.float32
        )
        first += sum(b.shape[0] for b in bufs)
    return total


def solution(mesh):
    finer = Mesh(mesh.devices.reshape(4, 4, 8, 2), ("y", "x", "z", "c"))
    every = SP + TP
    return jax.shard_map(
        body,
        mesh=finer,
        in_specs=(
            P(TP, SP),
            P(TP, SP),
            P(TP, SP),
            P(SP),
            P(TP, None),
            P(TP),
            P(TP, None),
            P(every, None),
            P(),
            P(every, None),
            P(every, None),
            P(SP, None, None),
            P(SP, None, None),
            P(SP, None, None),
        ),
        out_specs=P(every, None),
        check_vma=False,
    )
```

```python
import functools

import jax
import jax.numpy as jnp
import numpy as np
from jax import lax
from jax.experimental import pallas as pl
from jax.experimental.pallas import tpu as pltpu
from jax.sharding import Mesh
from jax.sharding import PartitionSpec as P


HEAD = 64
EPS = 1e-06
ROWS = 256
HALF = 128
SLOT = 32
CHUNK = 64
WIDTH = 2048
FF = 512
TILE = 512
SP = ("y", "x")
TP = ("z", "c")
CHIP = ("y", "x", "c")

PAIRS = (
    ((1, 2), (3, 2)),
    ((2, 1), (2, 3)),
    ((2, 2), (0, 0)),
    ((0, 2), (2, 0)),
    ((1, 1), (3, 3)),
    ((1, 3), (3, 1)),
    ((1, 0), (3, 0)),
    ((0, 1), (0, 3)),
)
GROUPS = ((0, 1), (2, 3), (4, 5), (6, 7))

VMEM = pl.BlockSpec(memory_space=pltpu.VMEM)
SMEM = pl.BlockSpec(memory_space=pltpu.SMEM)


def permute(value, axes, sizes, move):
    pairs = []
    for i in np.ndindex(*sizes):
        j = tuple(int(v) for v in np.mod(move(*i), sizes))
        pairs.append((int(np.ravel_multi_index(i, sizes)), int(np.ravel_multi_index(j, sizes))))
    return lax.ppermute(value, axes, pairs)


def displaced(value, op, sign, cross=0):
    def move(y, x, c):
        dy, dx = PAIRS[op][c]
        return (y + sign * dy, x + sign * dx, c + cross)

    return permute(value, CHIP, (4, 4, 2), move)


def along_z(value, step):
    return permute(value, "z", (8,), lambda z: (z + step,))


def swap_cores(value):
    return permute(value, "c", (2,), lambda c: (c + 1,))


def after(value, *others):
    return lax.optimization_barrier((value, *others))[0]


def in_hbm(value):
    return pltpu.with_memory_space_constraint(value, pltpu.HBM)


def cost(flops, nbytes):
    return pl.CostEstimate(flops=int(flops), bytes_accessed=int(nbytes), transcendentals=0)


def params(mib, grid=False):
    kwargs = {"dimension_semantics": ("arbitrary",)} if grid else {}
    return pltpu.CompilerParams(vmem_limit_bytes=mib << 20, **kwargs)


def conv_kernel(a_ref, b_ref, o_ref, m1_ref, m2_ref, halo_ref, taps_ref, gain_ref, out_ref, prev):
    @pl.when(pl.program_id(0) == 0)
    def _():
        prev[...] = halo_ref[...]

    lane = lax.broadcasted_iota(jnp.int32, (HEAD, ROWS), 1)
    t0, t1, t2 = taps_ref[:, 0:1], taps_ref[:, 1:2], taps_ref[:, 2:3]
    gain = gain_ref[...]
    g = prev[...]
    p1, p2 = pltpu.roll(g, 1, 1), pltpu.roll(g, 2, 1)
    for t in range(4):
        at = slice(t * ROWS, (t + 1) * ROWS)
        g = a_ref[:, at].astype(jnp.float32) * b_ref[:, at].astype(jnp.float32)
        r1, r2 = pltpu.roll(g, 1, 1), pltpu.roll(g, 2, 1)
        g1 = jnp.where(lane < 1, p1, r1)
        g2 = jnp.where(lane < 2, p2, r2)
        conv = t2 * g + t1 * (g1 * m1_ref[:, at]) + t0 * (g2 * m2_ref[:, at])
        v = o_ref[:, at].astype(jnp.float32) * conv
        ms = jnp.sum(v * v, axis=0, keepdims=True) * (1.0 / HEAD)
        out_ref[t] = (v * lax.rsqrt(ms + EPS) * gain).astype(jnp.bfloat16)
        p1, p2 = r1, r2
    prev[...] = g


def conv(conv_in, in_gate, out_gate, m1, m2, halo, taps, gain):
    wide = pl.BlockSpec((HEAD, 4 * ROWS), lambda i: (0, i))
    thin = pl.BlockSpec((1, 4 * ROWS), lambda i: (0, i))

    def whole(a):
        return pl.BlockSpec(a.shape, lambda i: (0, 0))

    return pl.pallas_call(
        conv_kernel,
        grid=(4,),
        out_shape=jax.ShapeDtypeStruct((16, HEAD, ROWS), jnp.bfloat16),
        in_specs=[wide, wide, wide, thin, thin, whole(halo), whole(taps), whole(gain)],
        out_specs=pl.BlockSpec((4, HEAD, ROWS), lambda i: (i, 0, 0)),
        scratch_shapes=[pltpu.VMEM((HEAD, ROWS), jnp.float32)],
        compiler_params=params(4, True),
        cost_estimate=cost(2e8, 2 << 20),
        name="conv",
    )(in_hbm(conv_in), in_hbm(in_gate), in_hbm(out_gate), m1, m2, halo, taps, gain)


OFFSETS = (0, -1, 1, -2, 2, -3, 3, -4)


def mix_kernel(where_ref, by_row_ref, *refs):
    n_own = len(OFFSETS)
    own = refs[:n_own]
    swapped = refs[n_own : n_own + 2]
    resid_ref, gain_ref, stream_ref, normed_ref, lhs, rhs, kept, total = refs[n_own + 2 :]
    z, c = where_ref[0], where_ref[1]
    step = pl.program_id(0)

    @pl.when(step == 0)
    def _():
        for q, off in enumerate(OFFSETS):
            zz = lax.rem(z + (off + 8), 8)
            lhs[pl.ds(q * 64, 64), :] = by_row_ref[zz * 2 + c]
            lhs[pl.ds(512 + q * 64, 64), :] = by_row_ref[zz * 2 + 1 - c]
        total[...] = jnp.zeros_like(total)

    row = 0
    for ref in (*own, *swapped):
        rhs[pl.ds(row, ref.shape[0]), :] = ref[...]
        row += ref.shape[0]
    mixed = lax.dot_general(
        lhs[...], rhs[...], (((0,), (0,)), ((), ())), preferred_element_type=jnp.float32
    )
    stream = resid_ref[...].astype(jnp.float32) + mixed
    stream_ref[...] = stream
    kept[step] = stream
    total[...] += jnp.broadcast_to(jnp.sum(stream * stream, axis=1, keepdims=True), total.shape)

    @pl.when(step == WIDTH // TILE - 1)
    def _():
        scale = lax.rsqrt(total[:, 0:1] * (1.0 / WIDTH) + EPS)
        for n in range(WIDTH // TILE):
            at = slice(n * TILE, (n + 1) * TILE)
            normed_ref[:, at] = (kept[n] * scale * gain_ref[:, at]).astype(jnp.bfloat16)


def mix(where, by_row, own, swapped, resid, gain):
    def tall(a):
        return pl.BlockSpec((a.shape[0], TILE), lambda i: (0, i))

    return pl.pallas_call(
        mix_kernel,
        grid=(WIDTH // TILE,),
        out_shape=[
            pltpu.HBM((ROWS, WIDTH), jnp.float32),
            jax.ShapeDtypeStruct((ROWS, WIDTH), jnp.bfloat16),
        ],
        in_specs=[SMEM, pl.BlockSpec(by_row.shape, lambda i: (0, 0, 0))]
        + [tall(a) for a in (*own, *swapped, resid)]
        + [pl.BlockSpec(gain.shape, lambda i: (0, 0))],
        out_specs=[
            pl.BlockSpec((ROWS, TILE), lambda i: (0, i)),
            pl.BlockSpec((ROWS, WIDTH), lambda i: (0, 0)),
        ],
        scratch_shapes=[
            pltpu.VMEM((1024, ROWS), jnp.bfloat16),
            pltpu.VMEM((1024, TILE), jnp.bfloat16),
            pltpu.VMEM((WIDTH // TILE, ROWS, TILE), jnp.float32),
            pltpu.VMEM((ROWS, 128), jnp.float32),
        ],
        compiler_params=params(16, True),
        cost_estimate=cost(1.1e9, 8 << 20),
        name="mix",
    )(where, by_row, *own, *swapped, in_hbm(resid), gain)


def pack_kernel(mine_ref, theirs_ref, mine_at_ref, theirs_at_ref, *refs):
    outs, table = refs[: len(PAIRS)], refs[len(PAIRS)]

    @pl.when(pl.program_id(0) == 0)
    def _():
        slot = lax.broadcasted_iota(jnp.int32, (CHUNK, ROWS), 0)
        for half, ref in enumerate((mine_at_ref, theirs_at_ref)):
            for k in range(len(PAIRS)):
                hit = slot == ref[k : k + 1, :]
                table[half, pl.ds(k * CHUNK, CHUNK), :] = jnp.where(hit, 1.0, 0.0).astype(
                    jnp.bfloat16
                )

    for half, ref in enumerate((mine_ref, theirs_ref)):
        packed = jnp.dot(table[half], ref[...], preferred_element_type=jnp.float32)
        packed = packed.astype(jnp.bfloat16)
        for k, out in enumerate(outs):
            out[pl.ds(half * CHUNK, CHUNK), :] = packed[k * CHUNK : (k + 1) * CHUNK]


def pack(mine, theirs, mine_at, theirs_at):
    block = pl.BlockSpec((ROWS, TILE), lambda i: (0, i))
    at = pl.BlockSpec(mine_at.shape, lambda i: (0, 0))
    n = len(PAIRS)
    return pl.pallas_call(
        pack_kernel,
        grid=(WIDTH // TILE,),
        out_shape=[jax.ShapeDtypeStruct((2 * CHUNK, WIDTH), jnp.bfloat16)] * n,
        in_specs=[block, block, at, at],
        out_specs=[pl.BlockSpec((2 * CHUNK, TILE), lambda i: (0, i))] * n,
        scratch_shapes=[pltpu.VMEM((2, n * CHUNK, ROWS), jnp.bfloat16)],
        compiler_params=params(12, True),
        cost_estimate=cost(1.1e9, 6 << 20),
        name="pack",
    )(mine, theirs, mine_at, theirs_at)


def expert_kernel(n, *refs):
    bufs, (wg, wu, wd) = refs[:n], refs[n : n + 3]
    outs, rows = refs[n + 3 : -1], refs[-1]
    row = 0
    for ref in bufs:
        rows[pl.ds(row, ref.shape[0]), :] = ref[...]
        row += ref.shape[0]
    x = rows[...]
    g = jnp.dot(x, wg[...], preferred_element_type=jnp.float32)
    u = jnp.dot(x, wu[...], preferred_element_type=jnp.float32)
    h = (g / (1.0 + jnp.exp(-g)) * u).astype(jnp.bfloat16)
    for n0 in range(0, WIDTH, TILE):
        at = slice(n0, n0 + TILE)
        y = jnp.dot(h, wd[:, at], preferred_element_type=jnp.float32).astype(jnp.bfloat16)
        row = 0
        for ref in outs:
            ref[:, at] = y[row : row + ref.shape[0]]
            row += ref.shape[0]


def experts(bufs, wg, wu, wd, apart):
    rows = sum(b.shape[0] for b in bufs)
    size = CHUNK if apart else 2 * CHUNK
    n_out = rows // size
    return pl.pallas_call(
        functools.partial(expert_kernel, len(bufs)),
        out_shape=[jax.ShapeDtypeStruct((size, WIDTH), jnp.bfloat16)] * n_out,
        in_specs=[VMEM] * (len(bufs) + 3),
        out_specs=[VMEM] * n_out,
        scratch_shapes=[pltpu.VMEM((rows, WIDTH), jnp.bfloat16)],
        compiler_params=params(18),
        cost_estimate=cost(6.0 * rows * WIDTH * FF, 8 << 20),
        name="experts",
    )(*bufs, wg, wu, wd)


def weighted(place, weight, first, count):
    slot = lax.broadcasted_iota(jnp.int32, (ROWS, count), 1) + first
    table = jnp.where(place[:, 0:1] == slot, weight[:, 0:1], 0.0) + jnp.where(
        place[:, 1:2] == slot, weight[:, 1:2], 0.0
    )
    high = table.astype(jnp.bfloat16)
    return high, (table - high.astype(jnp.float32)).astype(jnp.bfloat16)


def apply(tables, rows):
    return sum(jnp.dot(t, rows, preferred_element_type=jnp.float32) for t in tables)


def gather_kernel(n, acc_ref, place_ref, weight_ref, place2_ref, weight2_ref, *refs):
    bufs = refs[:n]
    mine_ref, theirs_ref, mine, theirs = refs[n:]
    for i, ref in enumerate(bufs):
        mine[pl.ds(i * CHUNK, CHUNK), :] = ref[:CHUNK]
        theirs[pl.ds(i * CHUNK, CHUNK), :] = ref[CHUNK:]
    count = n * CHUNK
    own = weighted(place_ref[...], weight_ref[...], 0, count)
    mine_ref[...] = acc_ref[...] + apply(own, mine[...])
    other = weighted(place2_ref[...], weight2_ref[...], 0, count)
    theirs_ref[...] = apply(other, theirs[...])


def gather(acc, place, weight, place2, weight2, bufs):
    n = len(bufs)
    block = pl.BlockSpec((ROWS, TILE), lambda i: (0, i))
    pair = pl.BlockSpec((ROWS, 2), lambda i: (0, 0))
    return pl.pallas_call(
        functools.partial(gather_kernel, n),
        grid=(WIDTH // TILE,),
        out_shape=[
            pltpu.HBM((ROWS, WIDTH), jnp.float32),
            jax.ShapeDtypeStruct((ROWS, WIDTH), jnp.float32),
        ],
        in_specs=[block] + [pair] * 4 + [pl.BlockSpec((2 * CHUNK, TILE), lambda i: (0, i))] * n,
        out_specs=[block, block],
        scratch_shapes=[pltpu.VMEM((n * CHUNK, TILE), jnp.bfloat16)] * 2,
        compiler_params=params(14, True),
        cost_estimate=cost(8.0 * ROWS * n * CHUNK * WIDTH, 10 << 20),
        name="gather",
    )(in_hbm(acc), place, weight, place2, weight2, *bufs)


def finish_kernel(first, n, acc_ref, more_ref, place_ref, weight_ref, *refs):
    bufs, out_ref, rows = refs[:n], refs[n], refs[n + 1]
    for i, ref in enumerate(bufs):
        rows[pl.ds(i * CHUNK, CHUNK), :] = ref[...]
    half = n // 2 * CHUNK
    mine = weighted(place_ref[...], weight_ref[...], first, half)
    theirs = weighted(place_ref[...], weight_ref[...], first + 8 * CHUNK, half)
    total = acc_ref[...] + more_ref[...]
    total = total + apply(mine, rows[:half]) + apply(theirs, rows[half:])
    out_ref[...] = total.astype(out_ref.dtype)


def finish(first, acc, more, place, weight, bufs):
    n = len(bufs)
    block = pl.BlockSpec((ROWS, TILE), lambda i: (0, i))
    pair = pl.BlockSpec((ROWS, 2), lambda i: (0, 0))
    return pl.pallas_call(
        functools.partial(finish_kernel, first, n),
        grid=(WIDTH // TILE,),
        out_shape=jax.ShapeDtypeStruct((ROWS, WIDTH), jnp.bfloat16),
        in_specs=[block, block, pair, pair]
        + [pl.BlockSpec((CHUNK, TILE), lambda i: (0, i))] * n,
        out_specs=block,
        scratch_shapes=[pltpu.VMEM((n * CHUNK, TILE), jnp.bfloat16)],
        compiler_params=params(12, True),
        cost_estimate=cost(4.0 * ROWS * n * CHUNK * WIDTH, 6 << 20),
        name="finish",
    )(in_hbm(acc), more, place, weight, *bufs)


def places(ids, expert_of):
    at0 = ids[0:1] == expert_of[:, None]
    at1 = ids[1:2] == expert_of[:, None]
    named = at0 | at1
    position = np.arange(ROWS)
    earlier = (position[:, None] < position[None, :]) & (
        position[:, None] // HALF == position[None, :] // HALF
    )
    rank = jnp.dot(
        named.astype(jnp.bfloat16),
        jnp.asarray(earlier, jnp.bfloat16),
        preferred_element_type=jnp.float32,
    ).astype(jnp.int32)
    in_chunk = rank + jnp.asarray(position // HALF * SLOT, jnp.int32)[None]
    rows = jnp.where(named, in_chunk, -1)
    count = expert_of.shape[0]
    in_all = in_chunk + 1 + jnp.arange(count, dtype=jnp.int32)[:, None] * CHUNK
    place = jnp.stack(
        [jnp.sum(jnp.where(at, in_all, 0), axis=0) - 1 for at in (at0, at1)], axis=1
    )
    return rows, place


def body(
    conv_in,
    in_gate,
    out_gate,
    doc_ids,
    conv_taps,
    head_gain,
    out_proj,
    resid,
    norm_gain,
    route_ids,
    route_weight,
    w_gate,
    w_up,
    w_down,
):
    y, x, z, c = (lax.axis_index(a) for a in ("y", "x", "z", "c"))

    last = in_gate[:, -2:].astype(jnp.float32) * conv_in[:, -2:].astype(jnp.float32)
    doc_value = doc_ids.astype(jnp.float32)
    tail = jnp.concatenate([last, doc_value[None, -2:]], axis=0)
    halo = lax.ppermute(tail, SP, [(i, i + 1) for i in range(15)])

    plus, minus = [out_proj], [out_proj]
    plus.append(along_z(out_proj, 1))
    minus.append(along_z(out_proj, -1))

    doc_before = jnp.concatenate([halo[HEAD], doc_value])
    same_one = (doc_before[1:-1] == doc_value).astype(jnp.float32)[None]
    same_two = (doc_before[:-2] == doc_value).astype(jnp.float32)[None]
    before = jnp.pad(halo[:HEAD], ((0, 0), (ROWS - 2, 0)))
    head_normed = conv(
        conv_in, in_gate, out_gate, same_one, same_two, before, conv_taps, head_gain[:, None]
    )
    by_row = lax.all_to_all(head_normed, TP, split_axis=0, concat_axis=0, tiled=True)

    plus[1], minus[1] = after(plus[1], head_normed), after(minus[1], head_normed)
    for _ in range(2, 5):
        plus.append(along_z(plus[-1], 1))
    for _ in range(2, 4):
        minus.append(along_z(minus[-1], -1))
    own = [out_proj, plus[1], minus[1], plus[2], minus[2], plus[3], minus[3], plus[4]]
    swapped = [
        swap_cores(jnp.concatenate(own[:5], axis=0)),
        swap_cores(jnp.concatenate(own[5:], axis=0)),
    ]

    routes = jnp.concatenate([route_ids.astype(jnp.float32), route_weight], axis=1).T
    routes = after(routes, head_normed)
    other = swap_cores(routes)
    table = np.array(PAIRS, np.int32)
    first_core = jnp.asarray(table[:, 0])
    second_core = jnp.asarray(table[:, 1])
    mine_d = jnp.where(c == 0, first_core, second_core)
    theirs_d = jnp.where(c == 0, second_core, first_core)

    def numbers(d):
        return ((y + d[:, 0]) % 4) * 4 + (x + d[:, 1]) % 4

    experts_mine = numbers(mine_d)
    rows_mine, place = places(
        route_ids.T, jnp.concatenate([experts_mine, numbers(theirs_d)])
    )
    rows_theirs, place_theirs = places(other[:2].astype(jnp.int32), experts_mine)
    weight_theirs = other[2:].T

    where = jnp.stack([z, c]).astype(jnp.int32)
    stream, normed = mix(where, by_row, own, swapped, resid, norm_gain[None])
    sends = pack(normed, swap_cores(normed), rows_mine[:8], rows_theirs)
    arrived = [displaced(s, k, 1) for k, s in enumerate(sends)]

    wg, wu, wd = w_gate[0], w_up[0], w_down[0]
    back = []
    for n, group in enumerate(GROUPS):
        final = n == len(GROUPS) - 1
        inputs = [arrived[k] for k in group]
        results = experts(inputs, wg, wu, wd, final)
        if final:
            back += [displaced(results[2 * i], k, -1) for i, k in enumerate(group)]
            back += [displaced(results[2 * i + 1], k, -1, 1) for i, k in enumerate(group)]
        else:
            back += [displaced(r, k, -1) for r, k in zip(results, group)]
    total, partial = gather(
        stream, place, route_weight, place_theirs, weight_theirs, back[:6]
    )
    more = swap_cores(partial)
    return finish(6 * CHUNK, total, more, place, route_weight, back[6:])


def solution(mesh):
    finer = Mesh(mesh.devices.reshape(4, 4, 8, 2), ("y", "x", "z", "c"))
    every = SP + TP
    return jax.shard_map(
        body,
        mesh=finer,
        in_specs=(
            P(TP, SP),
            P(TP, SP),
            P(TP, SP),
            P(SP),
            P(TP, None),
            P(TP),
            P(TP, None),
            P(every, None),
            P(),
            P(every, None),
            P(every, None),
            P(SP, None, None),
            P(SP, None, None),
            P(SP, None, None),
        ),
        out_specs=P(every, None),
        check_vma=False,
    )
```

```python
import functools

import jax
import jax.numpy as jnp
import numpy as np
from jax import lax
from jax.experimental import pallas as pl
from jax.experimental.pallas import tpu as pltpu
from jax.sharding import Mesh
from jax.sharding import PartitionSpec as P


HEAD = 64
EPS = 1e-06
ROWS = 256
HALF = 128
SLOT = 32
CHUNK = 64
WIDTH = 2048
FF = 512
TILE = 512
SP = ("y", "x")
TP = ("z", "c")
CHIP = ("y", "x", "c")

PAIRS = (
    ((0, 0), (0, 0)),
    ((1, 1), (0, 2)),
    ((1, 3), (1, 1)),
    ((0, 2), (1, 3)),
    ((0, 1), (0, 3)),
    ((0, 3), (0, 1)),
    ((1, 0), (3, 0)),
    ((3, 0), (1, 0)),
)
EXPERTS_AT = np.array([[a, (b[0] + 2, b[1] + 2)] for a, b in PAIRS], np.int32) % 4
assert len({tuple(d) for pair in EXPERTS_AT.tolist() for d in pair}) == 16
GROUPS = ((0, 1), (2, 3), (4, 5), (6, 7))

VMEM = pl.BlockSpec(memory_space=pltpu.VMEM)
SMEM = pl.BlockSpec(memory_space=pltpu.SMEM)


def permute(value, axes, sizes, move):
    pairs = []
    for i in np.ndindex(*sizes):
        j = tuple(int(v) for v in np.mod(move(*i), sizes))
        pairs.append((int(np.ravel_multi_index(i, sizes)), int(np.ravel_multi_index(j, sizes))))
    return lax.ppermute(value, axes, pairs)


def displaced(value, op, sign, cross=0):
    def move(y, x, c):
        dy, dx = PAIRS[op][c]
        return (y + sign * dy, x + sign * dx, c + cross)

    if op == 0 and not cross:
        return value
    return permute(value, CHIP, (4, 4, 2), move)


def hosted(value):
    return permute(value, CHIP, (4, 4, 2), lambda y, x, c: (y - 2 * c, x - 2 * c, c))


def along_z(value, step):
    return permute(value, "z", (8,), lambda z: (z + step,))


def swap_cores(value):
    return permute(value, "c", (2,), lambda c: (c + 1,))


def after(value, *others):
    return lax.optimization_barrier((value, *others))[0]


def in_hbm(value):
    return pltpu.with_memory_space_constraint(value, pltpu.HBM)


def cost(flops, nbytes):
    return pl.CostEstimate(flops=int(flops), bytes_accessed=int(nbytes), transcendentals=0)


def params(mib, grid=False):
    kwargs = {"dimension_semantics": ("arbitrary",)} if grid else {}
    return pltpu.CompilerParams(vmem_limit_bytes=mib << 20, **kwargs)


def conv_kernel(a_ref, b_ref, o_ref, m1_ref, m2_ref, halo_ref, taps_ref, gain_ref, out_ref, prev):
    @pl.when(pl.program_id(0) == 0)
    def _():
        prev[...] = halo_ref[...]

    lane = lax.broadcasted_iota(jnp.int32, (HEAD, ROWS), 1)
    t0, t1, t2 = taps_ref[:, 0:1], taps_ref[:, 1:2], taps_ref[:, 2:3]
    gain = gain_ref[...]
    g = prev[...]
    p1, p2 = pltpu.roll(g, 1, 1), pltpu.roll(g, 2, 1)
    for t in range(4):
        at = slice(t * ROWS, (t + 1) * ROWS)
        g = a_ref[:, at].astype(jnp.float32) * b_ref[:, at].astype(jnp.float32)
        r1, r2 = pltpu.roll(g, 1, 1), pltpu.roll(g, 2, 1)
        g1 = jnp.where(lane < 1, p1, r1)
        g2 = jnp.where(lane < 2, p2, r2)
        conv = t2 * g + t1 * (g1 * m1_ref[:, at]) + t0 * (g2 * m2_ref[:, at])
        v = o_ref[:, at].astype(jnp.float32) * conv
        ms = jnp.sum(v * v, axis=0, keepdims=True) * (1.0 / HEAD)
        out_ref[t] = (v * lax.rsqrt(ms + EPS) * gain).astype(jnp.bfloat16)
        p1, p2 = r1, r2
    prev[...] = g


def conv(conv_in, in_gate, out_gate, m1, m2, halo, taps, gain):
    wide = pl.BlockSpec((HEAD, 4 * ROWS), lambda i: (0, i))
    thin = pl.BlockSpec((1, 4 * ROWS), lambda i: (0, i))

    def whole(a):
        return pl.BlockSpec(a.shape, lambda i: (0, 0))

    return pl.pallas_call(
        conv_kernel,
        grid=(4,),
        out_shape=jax.ShapeDtypeStruct((16, HEAD, ROWS), jnp.bfloat16),
        in_specs=[wide, wide, wide, thin, thin, whole(halo), whole(taps), whole(gain)],
        out_specs=pl.BlockSpec((4, HEAD, ROWS), lambda i: (i, 0, 0)),
        scratch_shapes=[pltpu.VMEM((HEAD, ROWS), jnp.float32)],
        compiler_params=params(4, True),
        cost_estimate=cost(2e8, 2 << 20),
        name="conv",
    )(in_hbm(conv_in), in_hbm(in_gate), in_hbm(out_gate), m1, m2, halo, taps, gain)


OFFSETS = (0, -1, 1, -2, 2, -3, 3, -4)


def mix_kernel(where_ref, by_row_ref, *refs):
    n_own = len(OFFSETS)
    own = refs[:n_own]
    swapped = refs[n_own : n_own + 2]
    resid_ref, gain_ref, stream_ref, normed_ref, lhs, rhs, kept, total = refs[n_own + 2 :]
    z, c = where_ref[0], where_ref[1]
    step = pl.program_id(0)

    @pl.when(step == 0)
    def _():
        for q, off in enumerate(OFFSETS):
            zz = lax.rem(z + (off + 8), 8)
            lhs[pl.ds(q * 64, 64), :] = by_row_ref[zz * 2 + c]
            lhs[pl.ds(512 + q * 64, 64), :] = by_row_ref[zz * 2 + 1 - c]
        total[...] = jnp.zeros_like(total)

    row = 0
    for ref in (*own, *swapped):
        rhs[pl.ds(row, ref.shape[0]), :] = ref[...]
        row += ref.shape[0]
    mixed = lax.dot_general(
        lhs[...], rhs[...], (((0,), (0,)), ((), ())), preferred_element_type=jnp.float32
    )
    stream = resid_ref[...].astype(jnp.float32) + mixed
    stream_ref[...] = stream
    kept[step] = stream
    total[...] += jnp.broadcast_to(jnp.sum(stream * stream, axis=1, keepdims=True), total.shape)

    @pl.when(step == WIDTH // TILE - 1)
    def _():
        scale = lax.rsqrt(total[:, 0:1] * (1.0 / WIDTH) + EPS)
        for n in range(WIDTH // TILE):
            at = slice(n * TILE, (n + 1) * TILE)
            normed_ref[:, at] = (kept[n] * scale * gain_ref[:, at]).astype(jnp.bfloat16)


def mix(where, by_row, own, swapped, resid, gain):
    def tall(a):
        return pl.BlockSpec((a.shape[0], TILE), lambda i: (0, i))

    return pl.pallas_call(
        mix_kernel,
        grid=(WIDTH // TILE,),
        out_shape=[
            pltpu.HBM((ROWS, WIDTH), jnp.float32),
            jax.ShapeDtypeStruct((ROWS, WIDTH), jnp.bfloat16),
        ],
        in_specs=[SMEM, pl.BlockSpec(by_row.shape, lambda i: (0, 0, 0))]
        + [tall(a) for a in (*own, *swapped, resid)]
        + [pl.BlockSpec(gain.shape, lambda i: (0, 0))],
        out_specs=[
            pl.BlockSpec((ROWS, TILE), lambda i: (0, i)),
            pl.BlockSpec((ROWS, WIDTH), lambda i: (0, 0)),
        ],
        scratch_shapes=[
            pltpu.VMEM((1024, ROWS), jnp.bfloat16),
            pltpu.VMEM((1024, TILE), jnp.bfloat16),
            pltpu.VMEM((WIDTH // TILE, ROWS, TILE), jnp.float32),
            pltpu.VMEM((ROWS, 128), jnp.float32),
        ],
        compiler_params=params(16, True),
        cost_estimate=cost(1.1e9, 8 << 20),
        name="mix",
    )(where, by_row, *own, *swapped, in_hbm(resid), gain)


def pack_kernel(mine_ref, theirs_ref, mine_at_ref, theirs_at_ref, *refs):
    outs, table = refs[: len(PAIRS)], refs[len(PAIRS)]

    @pl.when(pl.program_id(0) == 0)
    def _():
        slot = lax.broadcasted_iota(jnp.int32, (CHUNK, ROWS), 0)
        for half, ref in enumerate((mine_at_ref, theirs_at_ref)):
            for k in range(len(PAIRS)):
                hit = slot == ref[k : k + 1, :]
                table[half, pl.ds(k * CHUNK, CHUNK), :] = jnp.where(hit, 1.0, 0.0).astype(
                    jnp.bfloat16
                )

    for half, ref in enumerate((mine_ref, theirs_ref)):
        packed = jnp.dot(table[half], ref[...], preferred_element_type=jnp.float32)
        packed = packed.astype(jnp.bfloat16)
        for k, out in enumerate(outs):
            out[pl.ds(half * CHUNK, CHUNK), :] = packed[k * CHUNK : (k + 1) * CHUNK]


def pack(mine, theirs, mine_at, theirs_at):
    block = pl.BlockSpec((ROWS, TILE), lambda i: (0, i))
    at = pl.BlockSpec(mine_at.shape, lambda i: (0, 0))
    n = len(PAIRS)
    return pl.pallas_call(
        pack_kernel,
        grid=(WIDTH // TILE,),
        out_shape=[jax.ShapeDtypeStruct((2 * CHUNK, WIDTH), jnp.bfloat16)] * n,
        in_specs=[block, block, at, at],
        out_specs=[pl.BlockSpec((2 * CHUNK, TILE), lambda i: (0, i))] * n,
        scratch_shapes=[pltpu.VMEM((2, n * CHUNK, ROWS), jnp.bfloat16)],
        compiler_params=params(12, True),
        cost_estimate=cost(1.1e9, 6 << 20),
        name="pack",
    )(mine, theirs, mine_at, theirs_at)


def expert_kernel(n, *refs):
    bufs, (wg, wu, wd) = refs[:n], refs[n : n + 3]
    outs, rows = refs[n + 3 : -1], refs[-1]
    row = 0
    for ref in bufs:
        rows[pl.ds(row, ref.shape[0]), :] = ref[...]
        row += ref.shape[0]
    x = rows[...]
    g = jnp.dot(x, wg[...], preferred_element_type=jnp.float32)
    u = jnp.dot(x, wu[...], preferred_element_type=jnp.float32)
    h = (g / (1.0 + jnp.exp(-g)) * u).astype(jnp.bfloat16)
    for n0 in range(0, WIDTH, TILE):
        at = slice(n0, n0 + TILE)
        y = jnp.dot(h, wd[:, at], preferred_element_type=jnp.float32).astype(jnp.bfloat16)
        row = 0
        for ref in outs:
            ref[:, at] = y[row : row + ref.shape[0]]
            row += ref.shape[0]


def experts(bufs, wg, wu, wd, apart):
    rows = sum(b.shape[0] for b in bufs)
    size = CHUNK if apart else 2 * CHUNK
    n_out = rows // size
    return pl.pallas_call(
        functools.partial(expert_kernel, len(bufs)),
        out_shape=[jax.ShapeDtypeStruct((size, WIDTH), jnp.bfloat16)] * n_out,
        in_specs=[VMEM] * (len(bufs) + 3),
        out_specs=[VMEM] * n_out,
        scratch_shapes=[pltpu.VMEM((rows, WIDTH), jnp.bfloat16)],
        compiler_params=params(18),
        cost_estimate=cost(6.0 * rows * WIDTH * FF, 8 << 20),
        name="experts",
    )(*bufs, wg, wu, wd)


def weighted(place, weight, first, count):
    slot = lax.broadcasted_iota(jnp.int32, (ROWS, count), 1) + first
    table = jnp.where(place[:, 0:1] == slot, weight[:, 0:1], 0.0) + jnp.where(
        place[:, 1:2] == slot, weight[:, 1:2], 0.0
    )
    high = table.astype(jnp.bfloat16)
    return high, (table - high.astype(jnp.float32)).astype(jnp.bfloat16)


def apply(tables, rows):
    return sum(jnp.dot(t, rows, preferred_element_type=jnp.float32) for t in tables)


def gather_kernel(n, acc_ref, place_ref, weight_ref, place2_ref, weight2_ref, *refs):
    bufs = refs[:n]
    mine_ref, theirs_ref, mine, theirs = refs[n:]
    for i, ref in enumerate(bufs):
        mine[pl.ds(i * CHUNK, CHUNK), :] = ref[:CHUNK]
        theirs[pl.ds(i * CHUNK, CHUNK), :] = ref[CHUNK:]
    count = n * CHUNK
    own = weighted(place_ref[...], weight_ref[...], 0, count)
    mine_ref[...] = acc_ref[...] + apply(own, mine[...])
    other = weighted(place2_ref[...], weight2_ref[...], 0, count)
    theirs_ref[...] = apply(other, theirs[...]).astype(jnp.bfloat16)


def gather(acc, place, weight, place2, weight2, bufs):
    n = len(bufs)
    block = pl.BlockSpec((ROWS, TILE), lambda i: (0, i))
    pair = pl.BlockSpec((ROWS, 2), lambda i: (0, 0))
    return pl.pallas_call(
        functools.partial(gather_kernel, n),
        grid=(WIDTH // TILE,),
        out_shape=[
            pltpu.HBM((ROWS, WIDTH), jnp.float32),
            jax.ShapeDtypeStruct((ROWS, WIDTH), jnp.bfloat16),
        ],
        in_specs=[block] + [pair] * 4 + [pl.BlockSpec((2 * CHUNK, TILE), lambda i: (0, i))] * n,
        out_specs=[block, block],
        scratch_shapes=[pltpu.VMEM((n * CHUNK, TILE), jnp.bfloat16)] * 2,
        compiler_params=params(14, True),
        cost_estimate=cost(8.0 * ROWS * n * CHUNK * WIDTH, 10 << 20),
        name="gather",
    )(in_hbm(acc), place, weight, place2, weight2, *bufs)


def finish_kernel(first, n, acc_ref, more_ref, place_ref, weight_ref, *refs):
    bufs, out_ref, rows = refs[:n], refs[n], refs[n + 1]
    for i, ref in enumerate(bufs):
        rows[pl.ds(i * CHUNK, CHUNK), :] = ref[...]
    half = n // 2 * CHUNK
    mine = weighted(place_ref[...], weight_ref[...], first, half)
    theirs = weighted(place_ref[...], weight_ref[...], first + 8 * CHUNK, half)
    total = acc_ref[...] + more_ref[...].astype(jnp.float32)
    total = total + apply(mine, rows[:half]) + apply(theirs, rows[half:])
    out_ref[...] = total.astype(out_ref.dtype)


def finish(first, acc, more, place, weight, bufs):
    n = len(bufs)
    block = pl.BlockSpec((ROWS, TILE), lambda i: (0, i))
    pair = pl.BlockSpec((ROWS, 2), lambda i: (0, 0))
    return pl.pallas_call(
        functools.partial(finish_kernel, first, n),
        grid=(WIDTH // TILE,),
        out_shape=jax.ShapeDtypeStruct((ROWS, WIDTH), jnp.bfloat16),
        in_specs=[block, block, pair, pair]
        + [pl.BlockSpec((CHUNK, TILE), lambda i: (0, i))] * n,
        out_specs=block,
        scratch_shapes=[pltpu.VMEM((n * CHUNK, TILE), jnp.bfloat16)],
        compiler_params=params(12, True),
        cost_estimate=cost(4.0 * ROWS * n * CHUNK * WIDTH, 6 << 20),
        name="finish",
    )(in_hbm(acc), more, place, weight, *bufs)


def places(ids, expert_of):
    at0 = ids[0:1] == expert_of[:, None]
    at1 = ids[1:2] == expert_of[:, None]
    named = at0 | at1
    position = np.arange(ROWS)
    earlier = (position[:, None] < position[None, :]) & (
        position[:, None] // HALF == position[None, :] // HALF
    )
    rank = jnp.dot(
        named.astype(jnp.bfloat16),
        jnp.asarray(earlier, jnp.bfloat16),
        preferred_element_type=jnp.float32,
    ).astype(jnp.int32)
    in_chunk = rank + jnp.asarray(position // HALF * SLOT, jnp.int32)[None]
    rows = jnp.where(named, in_chunk, -1)
    count = expert_of.shape[0]
    in_all = in_chunk + 1 + jnp.arange(count, dtype=jnp.int32)[:, None] * CHUNK
    place = jnp.stack(
        [jnp.sum(jnp.where(at, in_all, 0), axis=0) - 1 for at in (at0, at1)], axis=1
    )
    return rows, place


def body(
    conv_in,
    in_gate,
    out_gate,
    doc_ids,
    conv_taps,
    head_gain,
    out_proj,
    resid,
    norm_gain,
    route_ids,
    route_weight,
    w_gate,
    w_up,
    w_down,
):
    y, x, z, c = (lax.axis_index(a) for a in ("y", "x", "z", "c"))

    wg = hosted(w_gate[0])
    wu = hosted(w_up[0])
    wd = hosted(w_down[0])

    last = in_gate[:, -2:].astype(jnp.float32) * conv_in[:, -2:].astype(jnp.float32)
    doc_value = doc_ids.astype(jnp.float32)
    tail = jnp.concatenate([last, doc_value[None, -2:]], axis=0)
    halo = lax.ppermute(tail, SP, [(i, i + 1) for i in range(15)])

    plus, minus = [out_proj], [out_proj]
    plus.append(along_z(out_proj, 1))
    minus.append(along_z(out_proj, -1))

    doc_before = jnp.concatenate([halo[HEAD], doc_value])
    same_one = (doc_before[1:-1] == doc_value).astype(jnp.float32)[None]
    same_two = (doc_before[:-2] == doc_value).astype(jnp.float32)[None]
    before = jnp.pad(halo[:HEAD], ((0, 0), (ROWS - 2, 0)))
    head_normed = conv(
        conv_in, in_gate, out_gate, same_one, same_two, before, conv_taps, head_gain[:, None]
    )
    by_row = lax.all_to_all(head_normed, TP, split_axis=0, concat_axis=0, tiled=True)

    plus[1], minus[1] = after(plus[1], head_normed), after(minus[1], head_normed)
    for _ in range(2, 5):
        plus.append(along_z(plus[-1], 1))
    for _ in range(2, 4):
        minus.append(along_z(minus[-1], -1))
    own = [out_proj, plus[1], minus[1], plus[2], minus[2], plus[3], minus[3], plus[4]]
    swapped = [
        swap_cores(jnp.concatenate(own[:5], axis=0)),
        swap_cores(jnp.concatenate(own[5:], axis=0)),
    ]

    routes = jnp.concatenate([route_ids.astype(jnp.float32), route_weight], axis=1).T
    routes = after(routes, head_normed)
    other = swap_cores(routes)
    first_core = jnp.asarray(EXPERTS_AT[:, 0])
    second_core = jnp.asarray(EXPERTS_AT[:, 1])
    mine_d = jnp.where(c == 0, first_core, second_core)
    theirs_d = jnp.where(c == 0, second_core, first_core)

    def numbers(d):
        return ((y + d[:, 0]) % 4) * 4 + (x + d[:, 1]) % 4

    experts_mine = numbers(mine_d)
    rows_mine, place = places(
        route_ids.T, jnp.concatenate([experts_mine, numbers(theirs_d)])
    )
    rows_theirs, place_theirs = places(other[:2].astype(jnp.int32), experts_mine)
    weight_theirs = other[2:].T

    where = jnp.stack([z, c]).astype(jnp.int32)
    stream, normed = mix(where, by_row, own, swapped, resid, norm_gain[None])
    normed_theirs = swap_cores(normed)
    sends = pack(normed, normed_theirs, rows_mine[:8], rows_theirs)
    arrived = [displaced(s, k, 1) for k, s in enumerate(sends)]

    back = []
    for n, group in enumerate(GROUPS):
        final = n == len(GROUPS) - 1
        inputs = [arrived[k] for k in group]
        results = experts(inputs, wg, wu, wd, final)
        if final:
            back += [displaced(results[2 * i], k, -1) for i, k in enumerate(group)]
            back += [displaced(results[2 * i + 1], k, -1, 1) for i, k in enumerate(group)]
        else:
            back += [displaced(r, k, -1) for r, k in zip(results, group)]
    total, partial = gather(
        stream, place, route_weight, place_theirs, weight_theirs, back[:6]
    )
    more = swap_cores(partial)
    return finish(6 * CHUNK, total, more, place, route_weight, back[6:])


def solution(mesh):
    finer = Mesh(mesh.devices.reshape(4, 4, 8, 2), ("y", "x", "z", "c"))
    every = SP + TP
    return jax.shard_map(
        body,
        mesh=finer,
        in_specs=(
            P(TP, SP),
            P(TP, SP),
            P(TP, SP),
            P(SP),
            P(TP, None),
            P(TP),
            P(TP, None),
            P(every, None),
            P(),
            P(every, None),
            P(every, None),
            P(SP, None, None),
            P(SP, None, None),
            P(SP, None, None),
        ),
        out_specs=P(every, None),
        check_vma=False,
    )
```

```python
import functools

import jax
import jax.numpy as jnp
import numpy as np
from jax import lax
from jax.experimental import pallas as pl
from jax.experimental.pallas import tpu as pltpu
from jax.sharding import Mesh
from jax.sharding import PartitionSpec as P


HEAD = 64
EPS = 1e-06
ROWS = 256
HALF = 128
SLOT = 32
CHUNK = 64
WIDTH = 2048
FF = 512
TILE = 512
SP = ("y", "x")
TP = ("z", "c")
CHIP = ("y", "x", "c")

PAIRS = (
    ((0, 1), (0, 3)),
    ((1, 0), (3, 0)),
    ((0, 3), (0, 1)),
    ((3, 0), (1, 0)),
    ((1, 1), (0, 2)),
    ((1, 3), (1, 1)),
    ((0, 2), (1, 3)),
    ((0, 0), (0, 0)),
)
LOCAL = 7
EXPERTS_AT = np.array([[a, (b[0] + 2, b[1] + 2)] for a, b in PAIRS], np.int32) % 4
assert len({tuple(d) for pair in EXPERTS_AT.tolist() for d in pair}) == 16
GROUPS = ((0, 1, 2, 3), (4, 7), (5, 6))

VMEM = pl.BlockSpec(memory_space=pltpu.VMEM)
SMEM = pl.BlockSpec(memory_space=pltpu.SMEM)


def permute(value, axes, sizes, move):
    pairs = []
    for i in np.ndindex(*sizes):
        j = tuple(int(v) for v in np.mod(move(*i), sizes))
        pairs.append((int(np.ravel_multi_index(i, sizes)), int(np.ravel_multi_index(j, sizes))))
    return lax.ppermute(value, axes, pairs)


def displaced(value, op, sign, cross=0):
    def move(y, x, c):
        dy, dx = PAIRS[op][c]
        return (y + sign * dy, x + sign * dx, c + cross)

    if op == LOCAL and not cross:
        return value
    return permute(value, CHIP, (4, 4, 2), move)


def hosted(value):
    return permute(value, CHIP, (4, 4, 2), lambda y, x, c: (y - 2 * c, x - 2 * c, c))


def along_z(value, step):
    return permute(value, "z", (8,), lambda z: (z + step,))


def swap_cores(value):
    return permute(value, "c", (2,), lambda c: (c + 1,))


def in_hbm(value):
    return pltpu.with_memory_space_constraint(value, pltpu.HBM)


def cost(flops, nbytes):
    return pl.CostEstimate(flops=int(flops), bytes_accessed=int(nbytes), transcendentals=0)


def params(mib, grid=False):
    kwargs = {"dimension_semantics": ("arbitrary",)} if grid else {}
    return pltpu.CompilerParams(vmem_limit_bytes=mib << 20, **kwargs)


def tail_kernel(a_ref, b_ref, doc_ref, out_ref):
    out_ref[:HEAD] = a_ref[...].astype(jnp.float32) * b_ref[...].astype(jnp.float32)
    out_ref[HEAD:] = jnp.broadcast_to(doc_ref[...].astype(jnp.float32), (8, 128))


def tail(conv_in, in_gate, docs):
    at = conv_in.shape[1] // 128 - 1
    wide = pl.BlockSpec((HEAD, 128), lambda i: (0, at))
    return pl.pallas_call(
        tail_kernel,
        grid=(1,),
        out_shape=jax.ShapeDtypeStruct((HEAD + 8, 128), jnp.float32),
        in_specs=[wide, wide, pl.BlockSpec((1, 128), lambda i: (0, at))],
        out_specs=pl.BlockSpec((HEAD + 8, 128), lambda i: (0, 0)),
        compiler_params=params(2, True),
        cost_estimate=cost(1e4, 1e5),
        name="tail",
    )(in_hbm(conv_in), in_hbm(in_gate), docs)


def conv_kernel(a_ref, b_ref, o_ref, doc_ref, halo_ref, small_ref, out_ref, prev):
    @pl.when(pl.program_id(0) == 0)
    def _():
        prev[:, :128] = halo_ref[...]
        prev[:, 128:] = halo_ref[...]

    lane = lax.broadcasted_iota(jnp.int32, (HEAD, ROWS), 1)
    small = small_ref[...].T
    t0, t1, t2, gain = (small[:HEAD, k : k + 1] for k in range(4))
    g, d = prev[:HEAD], prev[HEAD:]
    p1, p2 = pltpu.roll(g, 1, 1), pltpu.roll(g, 2, 1)
    d1, d2 = pltpu.roll(d, 1, 1), pltpu.roll(d, 2, 1)
    for t in range(4):
        at = slice(t * ROWS, (t + 1) * ROWS)
        g = a_ref[:, at].astype(jnp.float32) * b_ref[:, at].astype(jnp.float32)
        d = jnp.broadcast_to(doc_ref[:, at].astype(jnp.float32), (8, ROWS))
        r1, r2 = pltpu.roll(g, 1, 1), pltpu.roll(g, 2, 1)
        e1, e2 = pltpu.roll(d, 1, 1), pltpu.roll(d, 2, 1)
        m1 = jnp.where(jnp.where(lane[:8] < 1, d1, e1) == d, 1.0, 0.0)[0:1]
        m2 = jnp.where(jnp.where(lane[:8] < 2, d2, e2) == d, 1.0, 0.0)[0:1]
        g1 = jnp.where(lane < 1, p1, r1)
        g2 = jnp.where(lane < 2, p2, r2)
        conv = t2 * g + t1 * (g1 * m1) + t0 * (g2 * m2)
        v = o_ref[:, at].astype(jnp.float32) * conv
        ms = jnp.sum(v * v, axis=0, keepdims=True) * (1.0 / HEAD)
        out_ref[t] = (v * lax.rsqrt(ms + EPS) * gain).astype(jnp.bfloat16)
        p1, p2, d1, d2 = r1, r2, e1, e2
    prev[:HEAD] = g
    prev[HEAD:] = d


def conv(conv_in, in_gate, out_gate, docs, halo, small):
    wide = pl.BlockSpec((HEAD, 4 * ROWS), lambda i: (0, i))

    def whole(a):
        return pl.BlockSpec(a.shape, lambda i: (0, 0))

    return pl.pallas_call(
        conv_kernel,
        grid=(4,),
        out_shape=jax.ShapeDtypeStruct((16, HEAD, ROWS), jnp.bfloat16),
        in_specs=[wide] * 3
        + [pl.BlockSpec((1, 4 * ROWS), lambda i: (0, i)), whole(halo), whole(small)],
        out_specs=pl.BlockSpec((4, HEAD, ROWS), lambda i: (i, 0, 0)),
        scratch_shapes=[pltpu.VMEM((HEAD + 8, ROWS), jnp.float32)],
        compiler_params=params(4, True),
        cost_estimate=cost(2e8, 2 << 20),
        name="conv",
    )(in_hbm(conv_in), in_hbm(in_gate), in_hbm(out_gate), docs, halo, small)


def route_kernel(where_ref, mine_ref, other_ref, rows_ref, weights_ref, rows2_ref, weights2_ref):
    y, x, c = where_ref[0], where_ref[1], where_ref[3]
    n = len(PAIRS)
    lane = lax.broadcasted_iota(jnp.int32, (ROWS, ROWS), 1)
    line = lax.broadcasted_iota(jnp.int32, (ROWS, ROWS), 0)
    same = (line < HALF) == (lane < HALF)
    earlier = jnp.where((line < lane) & same, 1.0, 0.0).astype(jnp.bfloat16)
    base = jnp.where(lane[:1] < HALF, 0, SLOT)

    def places(route, sets, rows_out, weights_out):
        count = n * len(sets)
        line = lax.broadcasted_iota(jnp.int32, (count, ROWS), 0)
        number = jnp.zeros((count, ROWS), jnp.int32)
        for s, core in enumerate(sets):
            for k in range(n):
                dy = jnp.where(core == 0, int(EXPERTS_AT[k, 0, 0]), int(EXPERTS_AT[k, 1, 0]))
                dx = jnp.where(core == 0, int(EXPERTS_AT[k, 0, 1]), int(EXPERTS_AT[k, 1, 1]))
                e = lax.rem(y + dy, 4) * 4 + lax.rem(x + dx, 4)
                number = jnp.where(line == s * n + k, e, number)
        number = number.astype(jnp.float32)
        at0, at1 = number == route[0:1], number == route[1:2]
        named = jnp.where(at0 | at1, 1.0, 0.0)
        rank = jnp.dot(named.astype(jnp.bfloat16), earlier, preferred_element_type=jnp.float32)
        rows_out[...] = jnp.where(named > 0.0, rank.astype(jnp.int32) + base, -1)
        weights_out[...] = jnp.where(at0, route[2:3], 0.0) + jnp.where(at1, route[3:4], 0.0)

    places(mine_ref[...], (c, 1 - c), rows_ref, weights_ref)
    places(other_ref[...], (c,), rows2_ref, weights2_ref)


def route(where, mine, other):
    n = len(PAIRS)
    return pl.pallas_call(
        route_kernel,
        out_shape=[
            jax.ShapeDtypeStruct((count, ROWS), dtype)
            for count in (2 * n, n)
            for dtype in (jnp.int32, jnp.float32)
        ],
        in_specs=[SMEM, VMEM, VMEM],
        out_specs=[VMEM] * 4,
        compiler_params=params(2),
        cost_estimate=cost(1e7, 1e5),
        name="route",
    )(where, mine, other)


OFFSETS = (0, -1, 1, -2, 2, -3, 3, -4)


def mix_kernel(where_ref, by_row_ref, *refs):
    n_own = len(OFFSETS)
    own = refs[:n_own]
    swapped = refs[n_own : 2 * n_own]
    resid_ref, gain_ref, stream_ref, normed_ref, lhs, rhs, kept, total = refs[2 * n_own :]
    z, c = where_ref[2], where_ref[3]
    step = pl.program_id(0)

    @pl.when(step == 0)
    def _():
        for q, off in enumerate(OFFSETS):
            zz = lax.rem(z + (off + 8), 8)
            lhs[pl.ds(q * 64, 64), :] = by_row_ref[zz * 2 + c]
            lhs[pl.ds(512 + q * 64, 64), :] = by_row_ref[zz * 2 + 1 - c]
        total[...] = jnp.zeros_like(total)

    row = 0
    for ref in (*own, *swapped):
        rhs[pl.ds(row, ref.shape[0]), :] = ref[...]
        row += ref.shape[0]
    mixed = lax.dot_general(
        lhs[...], rhs[...], (((0,), (0,)), ((), ())), preferred_element_type=jnp.float32
    )
    stream = resid_ref[...].astype(jnp.float32) + mixed
    stream_ref[...] = stream
    kept[step] = stream
    total[...] += jnp.broadcast_to(jnp.sum(stream * stream, axis=1, keepdims=True), total.shape)

    @pl.when(step == WIDTH // TILE - 1)
    def _():
        scale = lax.rsqrt(total[:, 0:1] * (1.0 / WIDTH) + EPS)
        for n in range(WIDTH // TILE):
            at = slice(n * TILE, (n + 1) * TILE)
            normed_ref[:, at] = (kept[n] * scale * gain_ref[:, at]).astype(jnp.bfloat16)


def mix(where, by_row, own, swapped, resid, gain):
    def tall(a):
        return pl.BlockSpec((a.shape[0], TILE), lambda i: (0, i))

    return pl.pallas_call(
        mix_kernel,
        grid=(WIDTH // TILE,),
        out_shape=[
            pltpu.HBM((ROWS, WIDTH), jnp.float32),
            jax.ShapeDtypeStruct((ROWS, WIDTH), jnp.bfloat16),
        ],
        in_specs=[SMEM, pl.BlockSpec(by_row.shape, lambda i: (0, 0, 0))]
        + [tall(a) for a in (*own, *swapped, resid)]
        + [pl.BlockSpec(gain.shape, lambda i: (0, 0))],
        out_specs=[
            pl.BlockSpec((ROWS, TILE), lambda i: (0, i)),
            pl.BlockSpec((ROWS, WIDTH), lambda i: (0, 0)),
        ],
        scratch_shapes=[
            pltpu.VMEM((1024, ROWS), jnp.bfloat16),
            pltpu.VMEM((1024, TILE), jnp.bfloat16),
            pltpu.VMEM((WIDTH // TILE, ROWS, TILE), jnp.float32),
            pltpu.VMEM((ROWS, 128), jnp.float32),
        ],
        compiler_params=params(16, True),
        cost_estimate=cost(1.1e9, 8 << 20),
        name="mix",
    )(where, by_row, *own, *swapped, in_hbm(resid), gain)


def pack_kernel(mine_ref, theirs_ref, mine_at_ref, theirs_at_ref, *refs):
    outs, table = refs[: len(PAIRS)], refs[len(PAIRS)]

    @pl.when(pl.program_id(0) == 0)
    def _():
        slot = lax.broadcasted_iota(jnp.int32, (CHUNK, ROWS), 0)
        for half, ref in enumerate((mine_at_ref, theirs_at_ref)):
            for k in range(len(PAIRS)):
                hit = slot == ref[k : k + 1, :]
                table[half, pl.ds(k * CHUNK, CHUNK), :] = jnp.where(hit, 1.0, 0.0).astype(
                    jnp.bfloat16
                )

    for half, ref in enumerate((mine_ref, theirs_ref)):
        packed = jnp.dot(table[half], ref[...], preferred_element_type=jnp.float32)
        packed = packed.astype(jnp.bfloat16)
        for k, out in enumerate(outs):
            out[pl.ds(half * CHUNK, CHUNK), :] = packed[k * CHUNK : (k + 1) * CHUNK]


def pack(mine, theirs, mine_at, theirs_at):
    block = pl.BlockSpec((ROWS, TILE), lambda i: (0, i))
    at = pl.BlockSpec(mine_at.shape, lambda i: (0, 0))
    n = len(PAIRS)
    return pl.pallas_call(
        pack_kernel,
        grid=(WIDTH // TILE,),
        out_shape=[jax.ShapeDtypeStruct((2 * CHUNK, WIDTH), jnp.bfloat16)] * n,
        in_specs=[block, block, at, at],
        out_specs=[pl.BlockSpec((2 * CHUNK, TILE), lambda i: (0, i))] * n,
        scratch_shapes=[pltpu.VMEM((2, n * CHUNK, ROWS), jnp.bfloat16)],
        compiler_params=params(12, True),
        cost_estimate=cost(1.1e9, 6 << 20),
        name="pack",
    )(mine, theirs, mine_at, theirs_at)


def expert_kernel(n, *refs):
    bufs, (wg, wu, wd) = refs[:n], refs[n : n + 3]
    outs, rows = refs[n + 3 : -1], refs[-1]
    row = 0
    for ref in bufs:
        rows[pl.ds(row, ref.shape[0]), :] = ref[...]
        row += ref.shape[0]
    x = rows[...]
    g = jnp.dot(x, wg[...], preferred_element_type=jnp.float32)
    u = jnp.dot(x, wu[...], preferred_element_type=jnp.float32)
    h = (g / (1.0 + jnp.exp(-g)) * u).astype(jnp.bfloat16)
    for n0 in range(0, WIDTH, TILE):
        at = slice(n0, n0 + TILE)
        y = jnp.dot(h, wd[:, at], preferred_element_type=jnp.float32).astype(jnp.bfloat16)
        row = 0
        for ref in outs:
            ref[:, at] = y[row : row + ref.shape[0]]
            row += ref.shape[0]


def experts(bufs, wg, wu, wd, apart):
    rows = sum(b.shape[0] for b in bufs)
    size = CHUNK if apart else 2 * CHUNK
    n_out = rows // size
    return pl.pallas_call(
        functools.partial(expert_kernel, len(bufs)),
        out_shape=[jax.ShapeDtypeStruct((size, WIDTH), jnp.bfloat16)] * n_out,
        in_specs=[VMEM] * (len(bufs) + 3),
        out_specs=[VMEM] * n_out,
        scratch_shapes=[pltpu.VMEM((rows, WIDTH), jnp.bfloat16)],
        compiler_params=params(24),
        cost_estimate=cost(6.0 * rows * WIDTH * FF, 8 << 20),
        name="experts",
    )(*bufs, wg, wu, wd)


def tables(rows_ref, weights_ref, chunks, high, low):
    slot = lax.broadcasted_iota(jnp.int32, (CHUNK, ROWS), 0)
    for i, k in enumerate(chunks):
        table = jnp.where(slot == rows_ref[k : k + 1, :], weights_ref[k : k + 1, :], 0.0)
        top = table.astype(jnp.bfloat16)
        high[pl.ds(i * CHUNK, CHUNK), :] = top
        low[pl.ds(i * CHUNK, CHUNK), :] = (table - top.astype(jnp.float32)).astype(jnp.bfloat16)


def apply(high, low, rows):
    numbers = (((0,), (0,)), ((), ()))
    return sum(
        lax.dot_general(t[...], rows[...], numbers, preferred_element_type=jnp.float32)
        for t in (high, low)
    )


def gather_kernel(chunks, acc_ref, rows_ref, weights_ref, rows2_ref, weights2_ref, *refs):
    n = len(chunks)
    bufs = refs[:n]
    mine_ref, theirs_ref, mine, theirs, high, low, high2, low2 = refs[n:]

    @pl.when(pl.program_id(0) == 0)
    def _():
        tables(rows_ref, weights_ref, chunks, high, low)
        tables(rows2_ref, weights2_ref, chunks, high2, low2)

    for i, ref in enumerate(bufs):
        mine[pl.ds(i * CHUNK, CHUNK), :] = ref[:CHUNK]
        theirs[pl.ds(i * CHUNK, CHUNK), :] = ref[CHUNK:]
    mine_ref[...] = acc_ref[...] + apply(high, low, mine)
    theirs_ref[...] = apply(high2, low2, theirs).astype(jnp.bfloat16)


def gather(chunks, acc, rows, weights, rows2, weights2, bufs):
    n = len(chunks)
    block = pl.BlockSpec((ROWS, TILE), lambda i: (0, i))

    def whole(a):
        return pl.BlockSpec(a.shape, lambda i: (0, 0))

    return pl.pallas_call(
        functools.partial(gather_kernel, chunks),
        grid=(WIDTH // TILE,),
        out_shape=[
            pltpu.HBM((ROWS, WIDTH), jnp.float32),
            jax.ShapeDtypeStruct((ROWS, WIDTH), jnp.bfloat16),
        ],
        in_specs=[block]
        + [whole(a) for a in (rows, weights, rows2, weights2)]
        + [pl.BlockSpec((2 * CHUNK, TILE), lambda i: (0, i))] * n,
        out_specs=[block, block],
        scratch_shapes=[pltpu.VMEM((n * CHUNK, TILE), jnp.bfloat16)] * 2
        + [pltpu.VMEM((n * CHUNK, ROWS), jnp.bfloat16)] * 4,
        compiler_params=params(14, True),
        cost_estimate=cost(8.0 * ROWS * n * CHUNK * WIDTH, 10 << 20),
        name="gather",
    )(in_hbm(acc), rows, weights, rows2, weights2, *bufs)


def finish_kernel(chunks, acc_ref, more_ref, rows_ref, weights_ref, *refs):
    n = len(chunks)
    bufs = refs[:n]
    out_ref, rows, high, low = refs[n:]

    @pl.when(pl.program_id(0) == 0)
    def _():
        tables(rows_ref, weights_ref, chunks, high, low)

    for i, ref in enumerate(bufs):
        rows[pl.ds(i * CHUNK, CHUNK), :] = ref[...]
    total = acc_ref[...] + more_ref[...].astype(jnp.float32) + apply(high, low, rows)
    out_ref[...] = total.astype(out_ref.dtype)


def finish(chunks, acc, more, rows, weights, bufs):
    n = len(chunks)
    block = pl.BlockSpec((ROWS, TILE), lambda i: (0, i))

    def whole(a):
        return pl.BlockSpec(a.shape, lambda i: (0, 0))

    return pl.pallas_call(
        functools.partial(finish_kernel, chunks),
        grid=(WIDTH // TILE,),
        out_shape=jax.ShapeDtypeStruct((ROWS, WIDTH), jnp.bfloat16),
        in_specs=[block, block, whole(rows), whole(weights)]
        + [pl.BlockSpec((CHUNK, TILE), lambda i: (0, i))] * n,
        out_specs=block,
        scratch_shapes=[pltpu.VMEM((n * CHUNK, TILE), jnp.bfloat16)]
        + [pltpu.VMEM((n * CHUNK, ROWS), jnp.bfloat16)] * 2,
        compiler_params=params(12, True),
        cost_estimate=cost(4.0 * ROWS * n * CHUNK * WIDTH, 6 << 20),
        name="finish",
    )(in_hbm(acc), more, rows, weights, *bufs)


def body(
    conv_in,
    in_gate,
    out_gate,
    doc_ids,
    conv_taps,
    head_gain,
    out_proj,
    resid,
    norm_gain,
    route_ids,
    route_weight,
    w_gate,
    w_up,
    w_down,
):
    y, x, z, c = (lax.axis_index(a) for a in ("y", "x", "z", "c"))

    wg = hosted(w_gate[0])
    wu = hosted(w_up[0])
    wd = hosted(w_down[0])

    plus, minus = [out_proj], [out_proj]
    plus.append(along_z(out_proj, 1))
    minus.append(along_z(out_proj, -1))

    docs = doc_ids[None]
    last = tail(conv_in, in_gate, docs)
    halo = lax.ppermute(last, SP, [(i, i + 1) for i in range(15)])
    small = jnp.pad(jnp.concatenate([conv_taps.T, head_gain[None]]), ((0, 4), (0, 128 - HEAD)))
    head_normed = conv(conv_in, in_gate, out_gate, docs, halo, small)
    by_row = lax.all_to_all(head_normed, TP, split_axis=0, concat_axis=0, tiled=True)

    for _ in range(2, 5):
        plus.append(along_z(plus[-1], 1))
    for _ in range(2, 4):
        minus.append(along_z(minus[-1], -1))
    own = [out_proj, plus[1], minus[1], plus[2], minus[2], plus[3], minus[3], plus[4]]
    swapped = [swap_cores(w) for w in own]

    where = jnp.stack([y, x, z, c]).astype(jnp.int32)
    routes = jnp.concatenate([route_ids.astype(jnp.float32), route_weight], axis=1).T
    routes_other = swap_cores(routes)
    rows, weights, rows_other, weights_other = route(where, routes, routes_other)

    stream, normed = mix(where, by_row, own, swapped, resid, norm_gain[None])
    normed_other = swap_cores(normed)
    sends = pack(normed, normed_other, rows[: len(PAIRS)], rows_other)
    arrived = [displaced(s, k, 1) for k, s in enumerate(sends)]

    back, cross = {}, {}
    for n, group in enumerate(GROUPS):
        apart = n > 0
        inputs = [arrived[k] for k in group]
        results = experts(inputs, wg, wu, wd, apart)
        for i, k in enumerate(group):
            if apart:
                back[k] = displaced(results[2 * i], k, -1)
                cross[k] = displaced(results[2 * i + 1], k, -1, 1)
            else:
                back[k] = displaced(results[i], k, -1)
    near = GROUPS[0]
    far = [k for group in GROUPS[1:] for k in group]
    total, partial = gather(
        near, stream, rows, weights, rows_other, weights_other, [back[k] for k in near]
    )
    more = swap_cores(partial)
    chunks = tuple(far) + tuple(len(PAIRS) + k for k in far)
    return finish(
        chunks, total, more, rows, weights, [back[k] for k in far] + [cross[k] for k in far]
    )


def solution(mesh):
    finer = Mesh(mesh.devices.reshape(4, 4, 8, 2), ("y", "x", "z", "c"))
    every = SP + TP
    return jax.shard_map(
        body,
        mesh=finer,
        in_specs=(
            P(TP, SP),
            P(TP, SP),
            P(TP, SP),
            P(SP),
            P(TP, None),
            P(TP),
            P(TP, None),
            P(every, None),
            P(),
            P(every, None),
            P(every, None),
            P(SP, None, None),
            P(SP, None, None),
            P(SP, None, None),
        ),
        out_specs=P(every, None),
        check_vma=False,
    )
```

```python
import functools

import jax
import jax.numpy as jnp
import numpy as np
from jax import lax
from jax.experimental import pallas as pl
from jax.experimental.pallas import tpu as pltpu
from jax.sharding import Mesh
from jax.sharding import PartitionSpec as P


HEAD = 64
EPS = 1e-06
ROWS = 256
HALF = 128
SLOT = 32
CHUNK = 64
WIDTH = 2048
FF = 512
TILE = 512
SP = ("y", "x")
TP = ("z", "c")
CHIP = ("y", "x", "c")

PAIRS = (
    ((0, 1), (0, 3)),
    ((1, 0), (3, 0)),
    ((0, 3), (0, 1)),
    ((3, 0), (1, 0)),
    ((1, 1), (0, 2)),
    ((1, 3), (1, 1)),
    ((0, 2), (1, 3)),
    ((0, 0), (0, 0)),
)
LOCAL = 7
EXPERTS_AT = np.array([[a, (b[0] + 2, b[1] + 2)] for a, b in PAIRS], np.int32) % 4
assert len({tuple(d) for pair in EXPERTS_AT.tolist() for d in pair}) == 16
GROUPS = ((0, 1, 2, 3), (4, 7), (5, 6))

VMEM = pl.BlockSpec(memory_space=pltpu.VMEM)
SMEM = pl.BlockSpec(memory_space=pltpu.SMEM)


def permute(value, axes, sizes, move):
    pairs = []
    for i in np.ndindex(*sizes):
        j = tuple(int(v) for v in np.mod(move(*i), sizes))
        pairs.append((int(np.ravel_multi_index(i, sizes)), int(np.ravel_multi_index(j, sizes))))
    return lax.ppermute(value, axes, pairs)


def displaced(value, op, sign, cross=0):
    def move(y, x, c):
        dy, dx = PAIRS[op][c]
        return (y + sign * dy, x + sign * dx, c + cross)

    if op == LOCAL and not cross:
        return value
    return permute(value, CHIP, (4, 4, 2), move)


def hosted(value):
    pairs = []
    for y, x in np.ndindex(4, 4):
        to = (y + 2) % 4 * 4 + (x + 2) % 4
        pairs.append(((y * 4 + x) * 2 + 1, to * 2 + 1))
    return lax.ppermute(value, CHIP, pairs)


def along_z(value, step):
    return permute(value, "z", (8,), lambda z: (z + step,))


def swap_cores(value):
    return permute(value, "c", (2,), lambda c: (c + 1,))


def in_hbm(value):
    return pltpu.with_memory_space_constraint(value, pltpu.HBM)


def cost(flops, nbytes):
    return pl.CostEstimate(flops=int(flops), bytes_accessed=int(nbytes), transcendentals=0)


def params(mib, grid=False):
    kwargs = {"dimension_semantics": ("arbitrary",)} if grid else {}
    return pltpu.CompilerParams(vmem_limit_bytes=mib << 20, **kwargs)


def tail_kernel(a_ref, b_ref, doc_ref, out_ref):
    out_ref[:HEAD] = a_ref[...].astype(jnp.float32) * b_ref[...].astype(jnp.float32)
    out_ref[HEAD:] = jnp.broadcast_to(doc_ref[...].astype(jnp.float32), (8, 128))


def tail(conv_in, in_gate, docs):
    at = conv_in.shape[1] // 128 - 1
    wide = pl.BlockSpec((HEAD, 128), lambda i: (0, at))
    return pl.pallas_call(
        tail_kernel,
        grid=(1,),
        out_shape=jax.ShapeDtypeStruct((HEAD + 8, 128), jnp.float32),
        in_specs=[wide, wide, pl.BlockSpec((1, 128), lambda i: (0, at))],
        out_specs=pl.BlockSpec((HEAD + 8, 128), lambda i: (0, 0)),
        compiler_params=params(2, True),
        cost_estimate=cost(1e4, 1e5),
        name="tail",
    )(in_hbm(conv_in), in_hbm(in_gate), docs)


def conv_kernel(a_ref, b_ref, o_ref, doc_ref, halo_ref, small_ref, out_ref, prev):
    @pl.when(pl.program_id(0) == 0)
    def _():
        prev[:, :128] = halo_ref[...]
        prev[:, 128:] = halo_ref[...]

    lane = lax.broadcasted_iota(jnp.int32, (HEAD, ROWS), 1)
    small = small_ref[...].T
    t0, t1, t2, gain = (small[:HEAD, k : k + 1] for k in range(4))
    g, d = prev[:HEAD], prev[HEAD:]
    p1, p2 = pltpu.roll(g, 1, 1), pltpu.roll(g, 2, 1)
    d1, d2 = pltpu.roll(d, 1, 1), pltpu.roll(d, 2, 1)
    for t in range(4):
        at = slice(t * ROWS, (t + 1) * ROWS)
        g = a_ref[:, at].astype(jnp.float32) * b_ref[:, at].astype(jnp.float32)
        d = jnp.broadcast_to(doc_ref[:, at].astype(jnp.float32), (8, ROWS))
        r1, r2 = pltpu.roll(g, 1, 1), pltpu.roll(g, 2, 1)
        e1, e2 = pltpu.roll(d, 1, 1), pltpu.roll(d, 2, 1)
        m1 = jnp.where(jnp.where(lane[:8] < 1, d1, e1) == d, 1.0, 0.0)[0:1]
        m2 = jnp.where(jnp.where(lane[:8] < 2, d2, e2) == d, 1.0, 0.0)[0:1]
        g1 = jnp.where(lane < 1, p1, r1)
        g2 = jnp.where(lane < 2, p2, r2)
        conv = t2 * g + t1 * (g1 * m1) + t0 * (g2 * m2)
        v = o_ref[:, at].astype(jnp.float32) * conv
        ms = jnp.sum(v * v, axis=0, keepdims=True) * (1.0 / HEAD)
        out_ref[t] = (v * lax.rsqrt(ms + EPS) * gain).astype(jnp.bfloat16)
        p1, p2, d1, d2 = r1, r2, e1, e2
    prev[:HEAD] = g
    prev[HEAD:] = d


def conv(conv_in, in_gate, out_gate, docs, halo, small):
    wide = pl.BlockSpec((HEAD, 4 * ROWS), lambda i: (0, i))

    def whole(a):
        return pl.BlockSpec(a.shape, lambda i: (0, 0))

    return pl.pallas_call(
        conv_kernel,
        grid=(4,),
        out_shape=jax.ShapeDtypeStruct((16, HEAD, ROWS), jnp.bfloat16),
        in_specs=[wide] * 3
        + [pl.BlockSpec((1, 4 * ROWS), lambda i: (0, i)), whole(halo), whole(small)],
        out_specs=pl.BlockSpec((4, HEAD, ROWS), lambda i: (i, 0, 0)),
        scratch_shapes=[pltpu.VMEM((HEAD + 8, ROWS), jnp.float32)],
        compiler_params=params(4, True),
        cost_estimate=cost(2e8, 2 << 20),
        name="conv",
    )(in_hbm(conv_in), in_hbm(in_gate), in_hbm(out_gate), docs, halo, small)


def route_kernel(where_ref, mine_ref, other_ref, rows_ref, weights_ref, rows2_ref, weights2_ref):
    y, x, c = where_ref[0], where_ref[1], where_ref[3]
    n = len(PAIRS)
    lane = lax.broadcasted_iota(jnp.int32, (ROWS, ROWS), 1)
    line = lax.broadcasted_iota(jnp.int32, (ROWS, ROWS), 0)
    same = (line < HALF) == (lane < HALF)
    earlier = jnp.where((line < lane) & same, 1.0, 0.0).astype(jnp.bfloat16)
    base = jnp.where(lane[:1] < HALF, 0, SLOT)

    def places(route, sets, rows_out, weights_out):
        count = n * len(sets)
        line = lax.broadcasted_iota(jnp.int32, (count, ROWS), 0)
        number = jnp.zeros((count, ROWS), jnp.int32)
        for s, core in enumerate(sets):
            for k in range(n):
                dy = jnp.where(core == 0, int(EXPERTS_AT[k, 0, 0]), int(EXPERTS_AT[k, 1, 0]))
                dx = jnp.where(core == 0, int(EXPERTS_AT[k, 0, 1]), int(EXPERTS_AT[k, 1, 1]))
                e = lax.rem(y + dy, 4) * 4 + lax.rem(x + dx, 4)
                number = jnp.where(line == s * n + k, e, number)
        number = number.astype(jnp.float32)
        at0, at1 = number == route[0:1], number == route[1:2]
        named = jnp.where(at0 | at1, 1.0, 0.0)
        rank = jnp.dot(named.astype(jnp.bfloat16), earlier, preferred_element_type=jnp.float32)
        rows_out[...] = jnp.where(named > 0.0, rank.astype(jnp.int32) + base, -1)
        weights_out[...] = jnp.where(at0, route[2:3], 0.0) + jnp.where(at1, route[3:4], 0.0)

    places(mine_ref[...], (c, 1 - c), rows_ref, weights_ref)
    places(other_ref[...], (c,), rows2_ref, weights2_ref)


def route(where, mine, other):
    n = len(PAIRS)
    return pl.pallas_call(
        route_kernel,
        out_shape=[
            jax.ShapeDtypeStruct((count, ROWS), dtype)
            for count in (2 * n, n)
            for dtype in (jnp.int32, jnp.float32)
        ],
        in_specs=[SMEM, VMEM, VMEM],
        out_specs=[VMEM] * 4,
        compiler_params=params(2),
        cost_estimate=cost(1e7, 1e5),
        name="route",
    )(where, mine, other)


OFFSETS = (0, -1, 1, -2, 2, -3, 3, -4)


def mix_kernel(where_ref, by_row_ref, *refs):
    n_own = len(OFFSETS)
    own = refs[:n_own]
    swapped = refs[n_own : 2 * n_own]
    resid_ref, gain_ref, stream_ref, normed_ref, lhs, rhs, kept, total = refs[2 * n_own :]
    z, c = where_ref[2], where_ref[3]
    step = pl.program_id(0)

    @pl.when(step == 0)
    def _():
        for q, off in enumerate(OFFSETS):
            zz = lax.rem(z + (off + 8), 8)
            lhs[pl.ds(q * 64, 64), :] = by_row_ref[zz * 2 + c]
            lhs[pl.ds(512 + q * 64, 64), :] = by_row_ref[zz * 2 + 1 - c]
        total[...] = jnp.zeros_like(total)

    row = 0
    for ref in (*own, *swapped):
        rhs[pl.ds(row, ref.shape[0]), :] = ref[...]
        row += ref.shape[0]
    mixed = lax.dot_general(
        lhs[...], rhs[...], (((0,), (0,)), ((), ())), preferred_element_type=jnp.float32
    )
    stream = resid_ref[...].astype(jnp.float32) + mixed
    stream_ref[...] = stream
    kept[step] = stream
    total[...] += jnp.broadcast_to(jnp.sum(stream * stream, axis=1, keepdims=True), total.shape)

    @pl.when(step == WIDTH // TILE - 1)
    def _():
        scale = lax.rsqrt(total[:, 0:1] * (1.0 / WIDTH) + EPS)
        for n in range(WIDTH // TILE):
            at = slice(n * TILE, (n + 1) * TILE)
            normed_ref[:, at] = (kept[n] * scale * gain_ref[:, at]).astype(jnp.bfloat16)


def mix(where, by_row, own, swapped, resid, gain):
    def tall(a):
        return pl.BlockSpec((a.shape[0], TILE), lambda i: (0, i))

    return pl.pallas_call(
        mix_kernel,
        grid=(WIDTH // TILE,),
        out_shape=[
            pltpu.HBM((ROWS, WIDTH), jnp.float32),
            jax.ShapeDtypeStruct((ROWS, WIDTH), jnp.bfloat16),
        ],
        in_specs=[SMEM, pl.BlockSpec(by_row.shape, lambda i: (0, 0, 0))]
        + [tall(a) for a in (*own, *swapped, resid)]
        + [pl.BlockSpec(gain.shape, lambda i: (0, 0))],
        out_specs=[
            pl.BlockSpec((ROWS, TILE), lambda i: (0, i)),
            pl.BlockSpec((ROWS, WIDTH), lambda i: (0, 0)),
        ],
        scratch_shapes=[
            pltpu.VMEM((1024, ROWS), jnp.bfloat16),
            pltpu.VMEM((1024, TILE), jnp.bfloat16),
            pltpu.VMEM((WIDTH // TILE, ROWS, TILE), jnp.float32),
            pltpu.VMEM((ROWS, 128), jnp.float32),
        ],
        compiler_params=params(16, True),
        cost_estimate=cost(1.1e9, 8 << 20),
        name="mix",
    )(where, by_row, *map(in_hbm, own), *map(in_hbm, swapped), in_hbm(resid), gain)


def pack_kernel(mine_ref, theirs_ref, mine_at_ref, theirs_at_ref, *refs):
    outs, table = refs[: len(PAIRS)], refs[len(PAIRS)]

    @pl.when(pl.program_id(0) == 0)
    def _():
        slot = lax.broadcasted_iota(jnp.int32, (CHUNK, ROWS), 0)
        for half, ref in enumerate((mine_at_ref, theirs_at_ref)):
            for k in range(len(PAIRS)):
                hit = slot == ref[k : k + 1, :]
                table[half, pl.ds(k * CHUNK, CHUNK), :] = jnp.where(hit, 1.0, 0.0).astype(
                    jnp.bfloat16
                )

    for half, ref in enumerate((mine_ref, theirs_ref)):
        packed = jnp.dot(table[half], ref[...], preferred_element_type=jnp.float32)
        packed = packed.astype(jnp.bfloat16)
        for k, out in enumerate(outs):
            out[pl.ds(half * CHUNK, CHUNK), :] = packed[k * CHUNK : (k + 1) * CHUNK]


def pack(mine, theirs, mine_at, theirs_at):
    block = pl.BlockSpec((ROWS, TILE), lambda i: (0, i))
    at = pl.BlockSpec(mine_at.shape, lambda i: (0, 0))
    n = len(PAIRS)
    return pl.pallas_call(
        pack_kernel,
        grid=(WIDTH // TILE,),
        out_shape=[jax.ShapeDtypeStruct((2 * CHUNK, WIDTH), jnp.bfloat16)] * n,
        in_specs=[block, block, at, at],
        out_specs=[pl.BlockSpec((2 * CHUNK, TILE), lambda i: (0, i))] * n,
        scratch_shapes=[pltpu.VMEM((2, n * CHUNK, ROWS), jnp.bfloat16)],
        compiler_params=params(12, True),
        cost_estimate=cost(1.1e9, 6 << 20),
        name="pack",
    )(mine, theirs, mine_at, theirs_at)


def choose_kernel(where_ref, *refs):
    own, received, outs, sems = refs[:3], refs[3:6], refs[6:9], refs[9]
    c = where_ref[3]

    @pl.when(c == 0)
    def _():
        for k in range(3):
            pltpu.make_async_copy(own[k], outs[k], sems.at[k]).start()

    @pl.when(c != 0)
    def _():
        for k in range(3):
            pltpu.make_async_copy(received[k], outs[k], sems.at[k]).start()

    for k in range(3):
        pltpu.make_async_copy(own[k], outs[k], sems.at[k]).wait()


def choose(where, own, received):
    return pl.pallas_call(
        choose_kernel,
        out_shape=[jax.ShapeDtypeStruct(w.shape, w.dtype) for w in own],
        in_specs=[SMEM] + [pl.BlockSpec(memory_space=pltpu.HBM)] * 6,
        out_specs=[VMEM] * 3,
        scratch_shapes=[pltpu.SemaphoreType.DMA((3,))],
        compiler_params=params(8),
        cost_estimate=cost(1e6, 12 << 20),
        name="choose",
    )(where, *map(in_hbm, own), *map(in_hbm, received))


def expert_kernel(n, *refs):
    bufs, (wg, wu, wd) = refs[:n], refs[n : n + 3]
    outs, rows = refs[n + 3 : -1], refs[-1]
    row = 0
    for ref in bufs:
        rows[pl.ds(row, ref.shape[0]), :] = ref[...]
        row += ref.shape[0]
    x = rows[...]
    g = jnp.dot(x, wg[...], preferred_element_type=jnp.float32)
    u = jnp.dot(x, wu[...], preferred_element_type=jnp.float32)
    h = (g / (1.0 + jnp.exp(-g)) * u).astype(jnp.bfloat16)
    for n0 in range(0, WIDTH, TILE):
        at = slice(n0, n0 + TILE)
        y = jnp.dot(h, wd[:, at], preferred_element_type=jnp.float32).astype(jnp.bfloat16)
        row = 0
        for ref in outs:
            ref[:, at] = y[row : row + ref.shape[0]]
            row += ref.shape[0]


def experts(bufs, wg, wu, wd, apart):
    rows = sum(b.shape[0] for b in bufs)
    size = CHUNK if apart else 2 * CHUNK
    n_out = rows // size
    return pl.pallas_call(
        functools.partial(expert_kernel, len(bufs)),
        out_shape=[jax.ShapeDtypeStruct((size, WIDTH), jnp.bfloat16)] * n_out,
        in_specs=[VMEM] * (len(bufs) + 3),
        out_specs=[VMEM] * n_out,
        scratch_shapes=[pltpu.VMEM((rows, WIDTH), jnp.bfloat16)],
        compiler_params=params(24),
        cost_estimate=cost(6.0 * rows * WIDTH * FF, 8 << 20),
        name="experts",
    )(*bufs, wg, wu, wd)


def tables(rows_ref, weights_ref, chunks, high, low):
    slot = lax.broadcasted_iota(jnp.int32, (CHUNK, ROWS), 0)
    for i, k in enumerate(chunks):
        table = jnp.where(slot == rows_ref[k : k + 1, :], weights_ref[k : k + 1, :], 0.0)
        top = table.astype(jnp.bfloat16)
        high[pl.ds(i * CHUNK, CHUNK), :] = top
        low[pl.ds(i * CHUNK, CHUNK), :] = (table - top.astype(jnp.float32)).astype(jnp.bfloat16)


def apply(high, low, rows):
    numbers = (((0,), (0,)), ((), ()))
    return sum(
        lax.dot_general(t[...], rows[...], numbers, preferred_element_type=jnp.float32)
        for t in (high, low)
    )


def gather_kernel(chunks, acc_ref, rows_ref, weights_ref, rows2_ref, weights2_ref, *refs):
    n = len(chunks)
    bufs = refs[:n]
    mine_ref, theirs_ref, mine, theirs, high, low, high2, low2 = refs[n:]

    @pl.when(pl.program_id(0) == 0)
    def _():
        tables(rows_ref, weights_ref, chunks, high, low)
        tables(rows2_ref, weights2_ref, chunks, high2, low2)

    for i, ref in enumerate(bufs):
        mine[pl.ds(i * CHUNK, CHUNK), :] = ref[:CHUNK]
        theirs[pl.ds(i * CHUNK, CHUNK), :] = ref[CHUNK:]
    mine_ref[...] = acc_ref[...] + apply(high, low, mine)
    theirs_ref[...] = apply(high2, low2, theirs).astype(jnp.bfloat16)


def gather(chunks, acc, rows, weights, rows2, weights2, bufs):
    n = len(chunks)
    block = pl.BlockSpec((ROWS, TILE), lambda i: (0, i))

    def whole(a):
        return pl.BlockSpec(a.shape, lambda i: (0, 0))

    return pl.pallas_call(
        functools.partial(gather_kernel, chunks),
        grid=(WIDTH // TILE,),
        out_shape=[
            pltpu.HBM((ROWS, WIDTH), jnp.float32),
            jax.ShapeDtypeStruct((ROWS, WIDTH), jnp.bfloat16),
        ],
        in_specs=[block]
        + [whole(a) for a in (rows, weights, rows2, weights2)]
        + [pl.BlockSpec((2 * CHUNK, TILE), lambda i: (0, i))] * n,
        out_specs=[block, block],
        scratch_shapes=[pltpu.VMEM((n * CHUNK, TILE), jnp.bfloat16)] * 2
        + [pltpu.VMEM((n * CHUNK, ROWS), jnp.bfloat16)] * 4,
        compiler_params=params(14, True),
        cost_estimate=cost(8.0 * ROWS * n * CHUNK * WIDTH, 10 << 20),
        name="gather",
    )(in_hbm(acc), rows, weights, rows2, weights2, *bufs)


def finish_kernel(chunks, acc_ref, more_ref, rows_ref, weights_ref, *refs):
    n = len(chunks)
    bufs = refs[:n]
    out_ref, rows, high, low = refs[n:]

    @pl.when(pl.program_id(0) == 0)
    def _():
        tables(rows_ref, weights_ref, chunks, high, low)

    for i, ref in enumerate(bufs):
        rows[pl.ds(i * CHUNK, CHUNK), :] = ref[...]
    total = acc_ref[...] + more_ref[...].astype(jnp.float32) + apply(high, low, rows)
    out_ref[...] = total.astype(out_ref.dtype)


def finish(chunks, acc, more, rows, weights, bufs):
    n = len(chunks)
    block = pl.BlockSpec((ROWS, TILE), lambda i: (0, i))

    def whole(a):
        return pl.BlockSpec(a.shape, lambda i: (0, 0))

    return pl.pallas_call(
        functools.partial(finish_kernel, chunks),
        grid=(WIDTH // TILE,),
        out_shape=jax.ShapeDtypeStruct((ROWS, WIDTH), jnp.bfloat16),
        in_specs=[block, block, whole(rows), whole(weights)]
        + [pl.BlockSpec((CHUNK, TILE), lambda i: (0, i))] * n,
        out_specs=block,
        scratch_shapes=[pltpu.VMEM((n * CHUNK, TILE), jnp.bfloat16)]
        + [pltpu.VMEM((n * CHUNK, ROWS), jnp.bfloat16)] * 2,
        compiler_params=params(12, True),
        cost_estimate=cost(4.0 * ROWS * n * CHUNK * WIDTH, 6 << 20),
        name="finish",
    )(in_hbm(acc), more, rows, weights, *bufs)


def body(
    conv_in,
    in_gate,
    out_gate,
    doc_ids,
    conv_taps,
    head_gain,
    out_proj,
    resid,
    norm_gain,
    route_ids,
    route_weight,
    w_gate,
    w_up,
    w_down,
):
    y, x, z, c = (lax.axis_index(a) for a in ("y", "x", "z", "c"))

    own_weights = (w_gate[0], w_up[0], w_down[0])
    received = [hosted(w) for w in own_weights]

    plus, minus = [out_proj], [out_proj]
    plus.append(along_z(out_proj, 1))
    minus.append(along_z(out_proj, -1))

    docs = doc_ids[None]
    last = tail(conv_in, in_gate, docs)
    halo = lax.ppermute(last, SP, [(i, i + 1) for i in range(15)])
    small = jnp.pad(jnp.concatenate([conv_taps.T, head_gain[None]]), ((0, 4), (0, 128 - HEAD)))
    head_normed = conv(conv_in, in_gate, out_gate, docs, halo, small)
    by_row = lax.all_to_all(head_normed, TP, split_axis=0, concat_axis=0, tiled=True)

    for _ in range(2, 5):
        plus.append(along_z(plus[-1], 1))
    for _ in range(2, 4):
        minus.append(along_z(minus[-1], -1))
    own = [out_proj, plus[1], minus[1], plus[2], minus[2], plus[3], minus[3], plus[4]]
    swapped = [swap_cores(w) for w in own]

    where = jnp.stack([y, x, z, c]).astype(jnp.int32)
    routes = jnp.concatenate([route_ids.astype(jnp.float32), route_weight], axis=1).T
    routes_other = swap_cores(routes)
    rows, weights, rows_other, weights_other = route(where, routes, routes_other)

    stream, normed = mix(where, by_row, own, swapped, resid, norm_gain[None])
    normed_other = swap_cores(normed)
    sends = pack(normed, normed_other, rows[: len(PAIRS)], rows_other)
    arrived = [displaced(s, k, 1) for k, s in enumerate(sends)]

    wg, wu, wd = choose(where, own_weights, received)
    back, cross = {}, {}
    for n, group in enumerate(GROUPS):
        apart = n > 0
        inputs = [arrived[k] for k in group]
        results = experts(inputs, wg, wu, wd, apart)
        for i, k in enumerate(group):
            if apart:
                back[k] = displaced(results[2 * i], k, -1)
                cross[k] = displaced(results[2 * i + 1], k, -1, 1)
            else:
                back[k] = displaced(results[i], k, -1)
    near = GROUPS[0]
    far = [k for group in GROUPS[1:] for k in group]
    total, partial = gather(
        near, stream, rows, weights, rows_other, weights_other, [back[k] for k in near]
    )
    more = swap_cores(partial)
    chunks = tuple(far) + tuple(len(PAIRS) + k for k in far)
    return finish(
        chunks, total, more, rows, weights, [back[k] for k in far] + [cross[k] for k in far]
    )


def solution(mesh):
    finer = Mesh(mesh.devices.reshape(4, 4, 8, 2), ("y", "x", "z", "c"))
    every = SP + TP
    return jax.shard_map(
        body,
        mesh=finer,
        in_specs=(
            P(TP, SP),
            P(TP, SP),
            P(TP, SP),
            P(SP),
            P(TP, None),
            P(TP),
            P(TP, None),
            P(every, None),
            P(),
            P(every, None),
            P(every, None),
            P(SP, None, None),
            P(SP, None, None),
            P(SP, None, None),
        ),
        out_specs=P(every, None),
        check_vma=False,
    )
```

```python
import functools

import jax
import jax.numpy as jnp
import numpy as np
from jax import lax
from jax.experimental import pallas as pl
from jax.experimental.pallas import tpu as pltpu
from jax.sharding import Mesh
from jax.sharding import PartitionSpec as P


HEAD = 64
EPS = 1e-06
ROWS = 256
HALF = 128
SLOT = 32
CHUNK = 64
WIDTH = 2048
FF = 512
TILE = 512
SP = ("y", "x")
TP = ("z", "c")
CHIP = ("y", "x", "c")

PAIRS = (
    ((0, 1), (0, 3)),
    ((1, 0), (3, 0)),
    ((0, 3), (0, 1)),
    ((3, 0), (1, 0)),
    ((1, 1), (0, 2)),
    ((1, 3), (1, 1)),
    ((0, 2), (1, 3)),
    ((0, 0), (0, 0)),
)
LOCAL = 7
EXPERTS_AT = np.array([[a, (b[0] + 2, b[1] + 2)] for a, b in PAIRS], np.int32) % 4
assert len({tuple(d) for pair in EXPERTS_AT.tolist() for d in pair}) == 16
GROUPS = ((0, 1, 2, 3), (4, 7), (5, 6))

VMEM = pl.BlockSpec(memory_space=pltpu.VMEM)
SMEM = pl.BlockSpec(memory_space=pltpu.SMEM)


def permute(value, axes, sizes, move):
    pairs = []
    for i in np.ndindex(*sizes):
        j = tuple(int(v) for v in np.mod(move(*i), sizes))
        pairs.append((int(np.ravel_multi_index(i, sizes)), int(np.ravel_multi_index(j, sizes))))
    return lax.ppermute(value, axes, pairs)


def displaced(value, op, sign, cross=0):
    def move(y, x, c):
        dy, dx = PAIRS[op][c]
        return (y + sign * dy, x + sign * dx, c + cross)

    if op == LOCAL and not cross:
        return value
    return permute(value, CHIP, (4, 4, 2), move)


def hosted(value):
    pairs = []
    for y, x in np.ndindex(4, 4):
        to = (y + 2) % 4 * 4 + (x + 2) % 4
        pairs.append(((y * 4 + x) * 2 + 1, to * 2 + 1))
    return lax.ppermute(value, CHIP, pairs)


def with_next_plane(value):
    pairs = [(z * 2 + 1, (z ^ 1) * 2 + 1) for z in range(8)]
    return lax.ppermute(value, TP, pairs)


def along_z(value, step):
    return permute(value, "z", (8,), lambda z: (z + step,))


def swap_cores(value):
    return permute(value, "c", (2,), lambda c: (c + 1,))


def in_hbm(value):
    return pltpu.with_memory_space_constraint(value, pltpu.HBM)


def cost(flops, nbytes):
    return pl.CostEstimate(flops=int(flops), bytes_accessed=int(nbytes), transcendentals=0)


def params(mib, grid=False):
    kwargs = {"dimension_semantics": ("arbitrary",)} if grid else {}
    return pltpu.CompilerParams(vmem_limit_bytes=mib << 20, **kwargs)


def tail_kernel(a_ref, b_ref, doc_ref, out_ref):
    out_ref[:HEAD] = a_ref[...].astype(jnp.float32) * b_ref[...].astype(jnp.float32)
    out_ref[HEAD:] = jnp.broadcast_to(doc_ref[...].astype(jnp.float32), (8, 128))


def tail(conv_in, in_gate, docs):
    at = conv_in.shape[1] // 128 - 1
    wide = pl.BlockSpec((HEAD, 128), lambda i: (0, at))
    return pl.pallas_call(
        tail_kernel,
        grid=(1,),
        out_shape=jax.ShapeDtypeStruct((HEAD + 8, 128), jnp.float32),
        in_specs=[wide, wide, pl.BlockSpec((1, 128), lambda i: (0, at))],
        out_specs=pl.BlockSpec((HEAD + 8, 128), lambda i: (0, 0)),
        compiler_params=params(2, True),
        cost_estimate=cost(1e4, 1e5),
        name="tail",
    )(in_hbm(conv_in), in_hbm(in_gate), docs)


def conv_kernel(a_ref, b_ref, o_ref, doc_ref, halo_ref, small_ref, out_ref, prev):
    @pl.when(pl.program_id(0) == 0)
    def _():
        prev[:, :128] = halo_ref[...]
        prev[:, 128:] = halo_ref[...]

    lane = lax.broadcasted_iota(jnp.int32, (HEAD, ROWS), 1)
    small = small_ref[...].T
    t0, t1, t2, gain = (small[:HEAD, k : k + 1] for k in range(4))
    g, d = prev[:HEAD], prev[HEAD:]
    p1, p2 = pltpu.roll(g, 1, 1), pltpu.roll(g, 2, 1)
    d1, d2 = pltpu.roll(d, 1, 1), pltpu.roll(d, 2, 1)
    for t in range(4):
        at = slice(t * ROWS, (t + 1) * ROWS)
        g = a_ref[:, at].astype(jnp.float32) * b_ref[:, at].astype(jnp.float32)
        d = jnp.broadcast_to(doc_ref[:, at].astype(jnp.float32), (8, ROWS))
        r1, r2 = pltpu.roll(g, 1, 1), pltpu.roll(g, 2, 1)
        e1, e2 = pltpu.roll(d, 1, 1), pltpu.roll(d, 2, 1)
        m1 = jnp.where(jnp.where(lane[:8] < 1, d1, e1) == d, 1.0, 0.0)[0:1]
        m2 = jnp.where(jnp.where(lane[:8] < 2, d2, e2) == d, 1.0, 0.0)[0:1]
        g1 = jnp.where(lane < 1, p1, r1)
        g2 = jnp.where(lane < 2, p2, r2)
        conv = t2 * g + t1 * (g1 * m1) + t0 * (g2 * m2)
        v = o_ref[:, at].astype(jnp.float32) * conv
        ms = jnp.sum(v * v, axis=0, keepdims=True) * (1.0 / HEAD)
        out_ref[t] = (v * lax.rsqrt(ms + EPS) * gain).astype(jnp.bfloat16)
        p1, p2, d1, d2 = r1, r2, e1, e2
    prev[:HEAD] = g
    prev[HEAD:] = d


def conv(conv_in, in_gate, out_gate, docs, halo, small):
    wide = pl.BlockSpec((HEAD, 4 * ROWS), lambda i: (0, i))

    def whole(a):
        return pl.BlockSpec(a.shape, lambda i: (0, 0))

    return pl.pallas_call(
        conv_kernel,
        grid=(4,),
        out_shape=pltpu.HBM((16, HEAD, ROWS), jnp.bfloat16),
        in_specs=[wide] * 3
        + [pl.BlockSpec((1, 4 * ROWS), lambda i: (0, i)), whole(halo), whole(small)],
        out_specs=pl.BlockSpec((4, HEAD, ROWS), lambda i: (i, 0, 0)),
        scratch_shapes=[pltpu.VMEM((HEAD + 8, ROWS), jnp.float32)],
        compiler_params=params(4, True),
        cost_estimate=cost(2e8, 2 << 20),
        name="conv",
    )(in_hbm(conv_in), in_hbm(in_gate), in_hbm(out_gate), docs, halo, small)


def route_kernel(where_ref, mine_ref, other_ref, rows_ref, weights_ref, rows2_ref, weights2_ref):
    y, x, c = where_ref[0], where_ref[1], where_ref[3]
    n = len(PAIRS)
    lane = lax.broadcasted_iota(jnp.int32, (ROWS, ROWS), 1)
    line = lax.broadcasted_iota(jnp.int32, (ROWS, ROWS), 0)
    same = (line < HALF) == (lane < HALF)
    earlier = jnp.where((line < lane) & same, 1.0, 0.0).astype(jnp.bfloat16)
    base = jnp.where(lane[:1] < HALF, 0, SLOT)

    def places(route, sets, rows_out, weights_out):
        count = n * len(sets)
        line = lax.broadcasted_iota(jnp.int32, (count, ROWS), 0)
        number = jnp.zeros((count, ROWS), jnp.int32)
        for s, core in enumerate(sets):
            for k in range(n):
                dy = jnp.where(core == 0, int(EXPERTS_AT[k, 0, 0]), int(EXPERTS_AT[k, 1, 0]))
                dx = jnp.where(core == 0, int(EXPERTS_AT[k, 0, 1]), int(EXPERTS_AT[k, 1, 1]))
                e = lax.rem(y + dy, 4) * 4 + lax.rem(x + dx, 4)
                number = jnp.where(line == s * n + k, e, number)
        number = number.astype(jnp.float32)
        at0, at1 = number == route[0:1], number == route[1:2]
        named = jnp.where(at0 | at1, 1.0, 0.0)
        rank = jnp.dot(named.astype(jnp.bfloat16), earlier, preferred_element_type=jnp.float32)
        rows_out[...] = jnp.where(named > 0.0, rank.astype(jnp.int32) + base, -1)
        weights_out[...] = jnp.where(at0, route[2:3], 0.0) + jnp.where(at1, route[3:4], 0.0)

    places(mine_ref[...], (c, 1 - c), rows_ref, weights_ref)
    places(other_ref[...], (c,), rows2_ref, weights2_ref)


def route(where, mine, other):
    n = len(PAIRS)
    return pl.pallas_call(
        route_kernel,
        out_shape=[
            jax.ShapeDtypeStruct((count, ROWS), dtype)
            for count in (2 * n, n)
            for dtype in (jnp.int32, jnp.float32)
        ],
        in_specs=[SMEM, VMEM, VMEM],
        out_specs=[VMEM] * 4,
        compiler_params=params(2),
        cost_estimate=cost(1e7, 1e5),
        name="route",
    )(where, mine, other)


OFFSETS = (0, -1, 1, -2, 2, -3, 3, -4)


def mix_kernel(where_ref, by_row_ref, *refs):
    n_own = len(OFFSETS)
    own = refs[:n_own]
    swapped = refs[n_own : 2 * n_own]
    resid_ref, gain_ref, stream_ref, normed_ref, lhs, rhs, kept, total = refs[2 * n_own :]
    z, c = where_ref[2], where_ref[3]
    step = pl.program_id(0)

    @pl.when(step == 0)
    def _():
        for q, off in enumerate(OFFSETS):
            zz = lax.rem(z + (off + 8), 8)
            lhs[pl.ds(q * 64, 64), :] = by_row_ref[zz * 2 + c]
            lhs[pl.ds(512 + q * 64, 64), :] = by_row_ref[zz * 2 + 1 - c]
        total[...] = jnp.zeros_like(total)

    row = 0
    for ref in (*own, *swapped):
        rhs[pl.ds(row, ref.shape[0]), :] = ref[...]
        row += ref.shape[0]
    mixed = lax.dot_general(
        lhs[...], rhs[...], (((0,), (0,)), ((), ())), preferred_element_type=jnp.float32
    )
    stream = resid_ref[...].astype(jnp.float32) + mixed
    stream_ref[...] = stream
    kept[step] = stream
    total[...] += jnp.broadcast_to(jnp.sum(stream * stream, axis=1, keepdims=True), total.shape)

    @pl.when(step == WIDTH // TILE - 1)
    def _():
        scale = lax.rsqrt(total[:, 0:1] * (1.0 / WIDTH) + EPS)
        for n in range(WIDTH // TILE):
            at = slice(n * TILE, (n + 1) * TILE)
            normed_ref[:, at] = (kept[n] * scale * gain_ref[:, at]).astype(jnp.bfloat16)


def mix(where, by_row, own, swapped, resid, gain):
    def tall(a):
        return pl.BlockSpec((a.shape[0], TILE), lambda i: (0, i))

    return pl.pallas_call(
        mix_kernel,
        grid=(WIDTH // TILE,),
        out_shape=[
            pltpu.HBM((ROWS, WIDTH), jnp.float32),
            jax.ShapeDtypeStruct((ROWS, WIDTH), jnp.bfloat16),
        ],
        in_specs=[SMEM, pl.BlockSpec(by_row.shape, lambda i: (0, 0, 0))]
        + [tall(a) for a in (*own, *swapped, resid)]
        + [pl.BlockSpec(gain.shape, lambda i: (0, 0))],
        out_specs=[
            pl.BlockSpec((ROWS, TILE), lambda i: (0, i)),
            pl.BlockSpec((ROWS, WIDTH), lambda i: (0, 0)),
        ],
        scratch_shapes=[
            pltpu.VMEM((1024, ROWS), jnp.bfloat16),
            pltpu.VMEM((1024, TILE), jnp.bfloat16),
            pltpu.VMEM((WIDTH // TILE, ROWS, TILE), jnp.float32),
            pltpu.VMEM((ROWS, 128), jnp.float32),
        ],
        compiler_params=params(16, True),
        cost_estimate=cost(1.1e9, 8 << 20),
        name="mix",
    )(where, by_row, *map(in_hbm, own), *map(in_hbm, swapped), in_hbm(resid), gain)


def pack_kernel(mine_ref, theirs_ref, mine_at_ref, theirs_at_ref, *refs):
    outs, table = refs[: len(PAIRS)], refs[len(PAIRS)]

    @pl.when(pl.program_id(0) == 0)
    def _():
        slot = lax.broadcasted_iota(jnp.int32, (CHUNK, ROWS), 0)
        for half, ref in enumerate((mine_at_ref, theirs_at_ref)):
            for k in range(len(PAIRS)):
                hit = slot == ref[k : k + 1, :]
                table[half, pl.ds(k * CHUNK, CHUNK), :] = jnp.where(hit, 1.0, 0.0).astype(
                    jnp.bfloat16
                )

    for half, ref in enumerate((mine_ref, theirs_ref)):
        packed = jnp.dot(table[half], ref[...], preferred_element_type=jnp.float32)
        packed = packed.astype(jnp.bfloat16)
        for k, out in enumerate(outs):
            out[pl.ds(half * CHUNK, CHUNK), :] = packed[k * CHUNK : (k + 1) * CHUNK]


def pack(mine, theirs, mine_at, theirs_at):
    block = pl.BlockSpec((ROWS, TILE), lambda i: (0, i))
    at = pl.BlockSpec(mine_at.shape, lambda i: (0, 0))
    n = len(PAIRS)
    return pl.pallas_call(
        pack_kernel,
        grid=(WIDTH // TILE,),
        out_shape=[jax.ShapeDtypeStruct((2 * CHUNK, WIDTH), jnp.bfloat16)] * n,
        in_specs=[block, block, at, at],
        out_specs=[pl.BlockSpec((2 * CHUNK, TILE), lambda i: (0, i))] * n,
        scratch_shapes=[pltpu.VMEM((2, n * CHUNK, ROWS), jnp.bfloat16)],
        compiler_params=params(12, True),
        cost_estimate=cost(1.1e9, 6 << 20),
        name="pack",
    )(mine, theirs, mine_at, theirs_at)


BLOCK = 512


def down_blocks(down, out):
    return [
        (down.at[:, pl.ds(j * BLOCK, BLOCK)], out.at[pl.ds(j * FF, FF)])
        for j in range(WIDTH // BLOCK)
    ]


def row_blocks(value, out):
    rows = [pl.ds(j * BLOCK, BLOCK) for j in range(WIDTH // BLOCK)]
    return [(value.at[r], out.at[r]) for r in rows]


def copy_all(copies, sems):
    for k, (source, target) in enumerate(copies):
        pltpu.make_async_copy(source, target, sems.at[k]).start()
    for k, (source, target) in enumerate(copies):
        pltpu.make_async_copy(source, target, sems.at[k]).wait()


def pick_kernel(where_ref, gate, down, out, sems):
    odd = lax.rem(where_ref[2], 2)
    for which, copies in enumerate((row_blocks(gate, out), down_blocks(down, out))):

        @pl.when(odd == which)
        def _(copies=copies):
            copy_all(copies, sems)


def pick(where, gate, down):
    anywhere = pl.BlockSpec(memory_space=pl.ANY)
    return pl.pallas_call(
        pick_kernel,
        out_shape=jax.ShapeDtypeStruct((WIDTH, FF), gate.dtype),
        in_specs=[SMEM] + [anywhere] * 2,
        out_specs=VMEM,
        scratch_shapes=[pltpu.SemaphoreType.DMA((4,))],
        compiler_params=params(4),
        cost_estimate=cost(1e6, 4 << 20),
        name="pick",
    )(where, in_hbm(gate), in_hbm(down))


def choose_kernel(where_ref, gate, up, down, ours, traded, got_up, g_out, u_out, d_out, sems):
    odd, c = lax.rem(where_ref[2], 2), where_ref[3]
    own = row_blocks(gate, g_out) + row_blocks(up, u_out) + down_blocks(down, d_out)
    got = row_blocks(got_up, u_out)
    even_plane = row_blocks(ours, g_out) + row_blocks(traded, d_out) + got
    odd_plane = row_blocks(traded, g_out) + row_blocks(ours, d_out) + got
    for test, copies in (
        (c == 0, own),
        ((c != 0) & (odd == 0), even_plane),
        ((c != 0) & (odd != 0), odd_plane),
    ):

        @pl.when(test)
        def _(copies=copies):
            copy_all(copies, sems)


def choose(where, *weights):
    anywhere = pl.BlockSpec(memory_space=pl.ANY)
    return pl.pallas_call(
        choose_kernel,
        out_shape=[jax.ShapeDtypeStruct((WIDTH, FF), weights[0].dtype)] * 3,
        in_specs=[SMEM] + [anywhere] * 6,
        out_specs=[VMEM] * 3,
        scratch_shapes=[pltpu.SemaphoreType.DMA((12,))],
        compiler_params=params(8),
        cost_estimate=cost(1e6, 12 << 20),
        name="choose",
    )(where, *weights)


def expert_kernel(n, *refs):
    bufs, (gate, up, down) = refs[:n], refs[n : n + 3]
    outs, rows = refs[n + 3 : -1], refs[-1]
    row = 0
    for ref in bufs:
        rows[pl.ds(row, ref.shape[0]), :] = ref[...]
        row += ref.shape[0]
    g = jnp.dot(rows[...], gate[...], preferred_element_type=jnp.float32)
    u = jnp.dot(rows[...], up[...], preferred_element_type=jnp.float32)
    h = (g / (1.0 + jnp.exp(-g)) * u).astype(jnp.bfloat16)
    for j in range(WIDTH // BLOCK):
        at = slice(j * BLOCK, (j + 1) * BLOCK)
        part = down[j * FF : (j + 1) * FF]
        y = jnp.dot(h, part, preferred_element_type=jnp.float32).astype(jnp.bfloat16)
        row = 0
        for ref in outs:
            ref[:, at] = y[row : row + ref.shape[0]]
            row += ref.shape[0]


def experts(bufs, gate, up, down, apart):
    rows = sum(b.shape[0] for b in bufs)
    size = CHUNK if apart else 2 * CHUNK
    n_out = rows // size
    return pl.pallas_call(
        functools.partial(expert_kernel, len(bufs)),
        out_shape=[jax.ShapeDtypeStruct((size, WIDTH), jnp.bfloat16)] * n_out,
        in_specs=[VMEM] * (len(bufs) + 3),
        out_specs=[VMEM] * n_out,
        scratch_shapes=[pltpu.VMEM((rows, WIDTH), jnp.bfloat16)],
        compiler_params=params(24),
        cost_estimate=cost(6.0 * rows * WIDTH * FF, 8 << 20),
        name="experts",
    )(*bufs, gate, up, down)


def tables(rows_ref, weights_ref, chunks, high, low):
    slot = lax.broadcasted_iota(jnp.int32, (CHUNK, ROWS), 0)
    for i, k in enumerate(chunks):
        table = jnp.where(slot == rows_ref[k : k + 1, :], weights_ref[k : k + 1, :], 0.0)
        top = table.astype(jnp.bfloat16)
        high[pl.ds(i * CHUNK, CHUNK), :] = top
        low[pl.ds(i * CHUNK, CHUNK), :] = (table - top.astype(jnp.float32)).astype(jnp.bfloat16)


def apply(high, low, rows):
    numbers = (((0,), (0,)), ((), ()))
    return sum(
        lax.dot_general(t[...], rows[...], numbers, preferred_element_type=jnp.float32)
        for t in (high, low)
    )


def gather_kernel(chunks, acc_ref, rows_ref, weights_ref, rows2_ref, weights2_ref, *refs):
    n = len(chunks)
    bufs = refs[:n]
    mine_ref, theirs_ref, mine, theirs, high, low, high2, low2 = refs[n:]

    @pl.when(pl.program_id(0) == 0)
    def _():
        tables(rows_ref, weights_ref, chunks, high, low)
        tables(rows2_ref, weights2_ref, chunks, high2, low2)

    for i, ref in enumerate(bufs):
        mine[pl.ds(i * CHUNK, CHUNK), :] = ref[:CHUNK]
        theirs[pl.ds(i * CHUNK, CHUNK), :] = ref[CHUNK:]
    mine_ref[...] = acc_ref[...] + apply(high, low, mine)
    theirs_ref[...] = apply(high2, low2, theirs).astype(jnp.bfloat16)


def gather(chunks, acc, rows, weights, rows2, weights2, bufs):
    n = len(chunks)
    block = pl.BlockSpec((ROWS, TILE), lambda i: (0, i))

    def whole(a):
        return pl.BlockSpec(a.shape, lambda i: (0, 0))

    return pl.pallas_call(
        functools.partial(gather_kernel, chunks),
        grid=(WIDTH // TILE,),
        out_shape=[
            pltpu.HBM((ROWS, WIDTH), jnp.float32),
            jax.ShapeDtypeStruct((ROWS, WIDTH), jnp.bfloat16),
        ],
        in_specs=[block]
        + [whole(a) for a in (rows, weights, rows2, weights2)]
        + [pl.BlockSpec((2 * CHUNK, TILE), lambda i: (0, i))] * n,
        out_specs=[block, block],
        scratch_shapes=[pltpu.VMEM((n * CHUNK, TILE), jnp.bfloat16)] * 2
        + [pltpu.VMEM((n * CHUNK, ROWS), jnp.bfloat16)] * 4,
        compiler_params=params(14, True),
        cost_estimate=cost(8.0 * ROWS * n * CHUNK * WIDTH, 10 << 20),
        name="gather",
    )(in_hbm(acc), rows, weights, rows2, weights2, *bufs)


def finish_kernel(chunks, acc_ref, more_ref, rows_ref, weights_ref, *refs):
    n = len(chunks)
    bufs = refs[:n]
    out_ref, rows, high, low = refs[n:]

    @pl.when(pl.program_id(0) == 0)
    def _():
        tables(rows_ref, weights_ref, chunks, high, low)

    for i, ref in enumerate(bufs):
        rows[pl.ds(i * CHUNK, CHUNK), :] = ref[...]
    total = acc_ref[...] + more_ref[...].astype(jnp.float32) + apply(high, low, rows)
    out_ref[...] = total.astype(out_ref.dtype)


def finish(chunks, acc, more, rows, weights, bufs):
    n = len(chunks)
    block = pl.BlockSpec((ROWS, TILE), lambda i: (0, i))

    def whole(a):
        return pl.BlockSpec(a.shape, lambda i: (0, 0))

    return pl.pallas_call(
        functools.partial(finish_kernel, chunks),
        grid=(WIDTH // TILE,),
        out_shape=jax.ShapeDtypeStruct((ROWS, WIDTH), jnp.bfloat16),
        in_specs=[block, block, whole(rows), whole(weights)]
        + [pl.BlockSpec((CHUNK, TILE), lambda i: (0, i))] * n,
        out_specs=block,
        scratch_shapes=[pltpu.VMEM((n * CHUNK, TILE), jnp.bfloat16)]
        + [pltpu.VMEM((n * CHUNK, ROWS), jnp.bfloat16)] * 2,
        compiler_params=params(12, True),
        cost_estimate=cost(4.0 * ROWS * n * CHUNK * WIDTH, 6 << 20),
        name="finish",
    )(in_hbm(acc), more, rows, weights, *bufs)


def body(
    conv_in,
    in_gate,
    out_gate,
    doc_ids,
    conv_taps,
    head_gain,
    out_proj,
    resid,
    norm_gain,
    route_ids,
    route_weight,
    w_gate,
    w_up,
    w_down,
):
    y, x, z, c = (lax.axis_index(a) for a in ("y", "x", "z", "c"))

    where = jnp.stack([y, x, z, c]).astype(jnp.int32)
    own_weights = (w_gate[0], w_up[0], w_down[0])
    picked = pick(where, w_gate[0], w_down[0])
    ours = hosted(picked)
    traded = with_next_plane(ours)
    got_up = hosted(w_up[0])

    plus, minus = [out_proj], [out_proj]
    plus.append(along_z(out_proj, 1))
    minus.append(along_z(out_proj, -1))

    docs = doc_ids[None]
    last = tail(conv_in, in_gate, docs)
    halo = lax.ppermute(last, SP, [(i, i + 1) for i in range(15)])
    small = jnp.pad(jnp.concatenate([conv_taps.T, head_gain[None]]), ((0, 4), (0, 128 - HEAD)))
    head_normed = conv(conv_in, in_gate, out_gate, docs, halo, small)
    by_row = lax.all_to_all(head_normed, TP, split_axis=0, concat_axis=0, tiled=True)

    for _ in range(2, 5):
        plus.append(along_z(plus[-1], 1))
    for _ in range(2, 4):
        minus.append(along_z(minus[-1], -1))
    own = [out_proj, plus[1], minus[1], plus[2], minus[2], plus[3], minus[3], plus[4]]
    swapped = [swap_cores(w) for w in own]

    routes = jnp.concatenate([route_ids.astype(jnp.float32), route_weight], axis=1).T
    routes_other = swap_cores(routes)
    rows, weights, rows_other, weights_other = route(where, routes, routes_other)

    stream, normed = mix(where, by_row, own, swapped, resid, norm_gain[None])
    normed_other = swap_cores(normed)
    sends = pack(normed, normed_other, rows[: len(PAIRS)], rows_other)
    arrived = [displaced(s, k, 1) for k, s in enumerate(sends)]

    hosted_weights = choose(where, *own_weights, ours, traded, got_up)
    back, cross = {}, {}
    for n, group in enumerate(GROUPS):
        apart = n > 0
        inputs = [arrived[k] for k in group]
        results = experts(inputs, *hosted_weights, apart)
        for i, k in enumerate(group):
            if apart:
                back[k] = displaced(results[2 * i], k, -1)
                cross[k] = displaced(results[2 * i + 1], k, -1, 1)
            else:
                back[k] = displaced(results[i], k, -1)
    near = GROUPS[0]
    far = [k for group in GROUPS[1:] for k in group]
    total, partial = gather(
        near, stream, rows, weights, rows_other, weights_other, [back[k] for k in near]
    )
    more = swap_cores(partial)
    chunks = tuple(far) + tuple(len(PAIRS) + k for k in far)
    return finish(
        chunks, total, more, rows, weights, [back[k] for k in far] + [cross[k] for k in far]
    )


def solution(mesh):
    finer = Mesh(mesh.devices.reshape(4, 4, 8, 2), ("y", "x", "z", "c"))
    every = SP + TP
    return jax.shard_map(
        body,
        mesh=finer,
        in_specs=(
            P(TP, SP),
            P(TP, SP),
            P(TP, SP),
            P(SP),
            P(TP, None),
            P(TP),
            P(TP, None),
            P(every, None),
            P(),
            P(every, None),
            P(every, None),
            P(SP, None, None),
            P(SP, None, None),
            P(SP, None, None),
        ),
        out_specs=P(every, None),
        check_vma=False,
    )
```
